256 devices in a mesh: sp: 32 (over z, x), tp: 8 (over y, core).
Axes of the slice: x: 4, y: 4, z: 8, core: 2. Of those that a mesh axis runs over, the one named last changes fastest.
Arguments:
- block_input: bfloat16 [8192, 2048], P('sp'), may hold values from -12 to 12
- queries: bfloat16 [8192, 1024], P('sp', 'tp'), may hold values from -6 to 6
- keys: bfloat16 [8192, 1024], P('sp', 'tp'), may hold values from -6 to 6
- w_value: bfloat16 [2048, 2048], P(None, 'tp'), may hold values from -0.125 to 0.125
- log_decay: float32 [8192, 1024], P('sp', 'tp'), as said below
- d_out: bfloat16 [8192, 2048], P('sp', 'tp'), may hold values from -0.0625 to 0.0625
Outputs:
- d_queries: bfloat16 [8192, 1024], P('sp', 'tp')
- d_keys: bfloat16 [8192, 1024], P('sp', 'tp')
- d_log_decay: float32 [8192, 1024], P('sp', 'tp')
- d_w_value: float32 [2048, 2048], P('sp', 'tp')
- row_norms: float32 [2048], P('sp')
The draws below stay inside these ranges and needn't reach their ends.
Inputs may be any that keep to these rules, and one draw needn't show every extreme that they name: log_decay is negative; key channels differ in rate, and rates change along the sequence.
All inputs are finite; a program needn't handle non-finite values.
Results may differ from the reference program's by a relative error of at most 0.015.
Values sent between devices are 32-bit elements; how exact they have to be, the bound alone decides.
A program may use at most 64 MiB of HBM per device.

```python
import math
import jax
import jax.numpy as jnp
from jax import lax

D = 2048
HEADS = 8
DK = 128
DV = 256
TOK_DEV = 256
TOKENS = 8192


def draw_log_decay(key, part):
    rate_key, noise_key, span_key = jax.random.split(jax.random.fold_in(key, 11), 3)
    rates = jnp.exp(jax.random.uniform(rate_key, (HEADS * DK,), jnp.float32, math.log(0.08), math.log(2.1))) / TOKENS
    span_factor = jnp.exp(jax.random.uniform(span_key, (TOKENS // TOK_DEV, 1, HEADS * DK), jnp.float32, -1.5, 1.5))
    span_factor = jnp.broadcast_to(span_factor, (TOKENS // TOK_DEV, TOK_DEV, HEADS * DK)).reshape(TOKENS, HEADS * DK)
    noise = jnp.clip(0.5 * jax.random.normal(noise_key, (TOKENS, HEADS * DK), jnp.float32), -1.5, 1.5)
    return (-rates[None, :] * span_factor * jnp.exp(noise)).astype(jnp.float32)


def strengthened(values, key, source, target, shards_of, factor):
    def block_of(position):
        return (jnp.arange(values.shape[position]) // (values.shape[position] // shards_of)).reshape((-1,) + (1,) * (values.ndim - 1 - position))

    near = jax.random.permutation(key, shards_of)[block_of(target)]
    other_side = (block_of(target) + shards_of // 2) % shards_of
    return jnp.where((block_of(source) == near) | (block_of(source) == other_side), factor * values, values)


def levels(own_key, extent, shards, least, top_value):
    loudness, own = 1.0, jax.random.fold_in(own_key, 6)
    for dim, blocks in shards:
        draws = jnp.exp(jax.random.uniform(jax.random.fold_in(own, dim), (blocks,), jnp.float32, least / len(shards), top_value / len(shards)))
        loudness = loudness * jnp.repeat(draws, extent[dim] // blocks).reshape([-1 if axis == dim else 1 for axis in range(len(extent))])
    return loudness


def normal_values(own_key, dims, deviation, limit, cuts=(), kind=jnp.bfloat16):
    values = deviation * jax.random.normal(own_key, dims, jnp.float32)
    if cuts:
        values = values * levels(own_key, dims, cuts, -0.22, 0.18)
    return jnp.clip(values, -limit, limit).astype(kind)


def gaussian_with(stream_key, shape, spread, bound, cuts, heavy, held_as=jnp.bfloat16):
    values = spread * jax.random.normal(stream_key, shape, jnp.float32)
    if cuts:
        values = values * levels(stream_key, shape, cuts, -0.22, 0.18)
    return jnp.clip(strengthened(values, jax.random.fold_in(stream_key, 3), *heavy), -bound, bound).astype(held_as)


def setup_inputs(seed: int = 0) -> dict:
    key_list = jax.random.split(jax.random.key(seed), 7)
    block_input = gaussian_with(key_list[0], (TOKENS, D), 1.0, 12.0, ((0, 32),), (0, 1, 32, 2.75))
    queries = normal_values(key_list[1], (TOKENS, HEADS * DK), 1.0, 6.0, ((0, 32), (1, 8)))
    keys = normal_values(key_list[2], (TOKENS, HEADS * DK), 1.0, 6.0, ((0, 32), (1, 8)))
    w_value = normal_values(key_list[3], (D, HEADS * DV), D ** -0.5, 0.125, ((1, 8),))
    log_decay = draw_log_decay(jax.random.fold_in(key_list[6], 71), 0)
    d_out = normal_values(key_list[5], (TOKENS, HEADS * DV), (TOKENS ** -0.5), 0.0625, ((0, 32), (1, 8)))
    return dict(block_input=block_input, queries=queries, keys=keys, w_value=w_value, log_decay=log_decay, d_out=d_out)


def split_heads(array, block_len, width):
    length = array.shape[0]
    return array.reshape(length // block_len, block_len, -1, width).transpose(2, 0, 1, 3)


def merge_heads(array):
    return array.transpose(1, 2, 0, 3).reshape(array.shape[1] * array.shape[2], -1)


def product(form, left, right):
    return jnp.einsum(form, left.astype(jnp.float32), right.astype(jnp.float32), precision=lax.Precision.HIGHEST)


def reference(block_input, queries, keys, w_value, log_decay, d_out):
    q_scale = DK ** -0.5
    values = jnp.dot(block_input, w_value, preferred_element_type=jnp.float32).astype(jnp.bfloat16)
    block_len = 32
    q_heads = split_heads(queries, block_len, DK).astype(jnp.float32) * q_scale
    k_heads = split_heads(keys, block_len, DK).astype(jnp.float32)
    v_heads = split_heads(values, block_len, DV)
    g_heads = split_heads(log_decay, block_len, DK).astype(jnp.float32)
    o_grad = split_heads(d_out, block_len, DV)
    cumlog = jnp.cumsum(g_heads, axis=2)
    last_log = cumlog[:, :, -1:, :]
    k_tail = jnp.exp(last_log - cumlog)
    q_grown = (q_heads * jnp.exp(cumlog)).astype(jnp.bfloat16)
    k_shrunk = (k_heads * jnp.exp(-cumlog)).astype(jnp.bfloat16)
    k_tailed = (k_heads * k_tail).astype(jnp.bfloat16)
    causal = jnp.tril(jnp.ones((block_len, block_len), jnp.float32))
    out_dots = (product('hbcv,hbsv->hbcs', o_grad, v_heads) * causal).astype(jnp.bfloat16)
    key_dots = (product('hbcd,hbsd->hbcs', q_grown, k_shrunk) * causal).astype(jnp.bfloat16)
    increments = product('hbcd,hbcv->hbdv', k_tailed, v_heads)
    backwards = product('hbcd,hbcv->hbdv', q_grown, o_grad)
    block_decay = jnp.exp(last_log[:, :, 0, :])

    def leading(array):
        return jnp.moveaxis(array, 1, 0)

    def forward_step(carried, inputs):
        decay_block, grown = inputs
        return decay_block[:, :, None] * carried + grown, carried

    zero_state = jnp.zeros((HEADS, DK, DV), jnp.float32)
    _, entering = lax.scan(forward_step, zero_state, (leading(block_decay), leading(increments)))

    def backward_step(adjoint, inputs):
        decay_block, grown = inputs
        return grown + decay_block[:, :, None] * adjoint, adjoint

    _, from_right = lax.scan(backward_step, zero_state, (leading(block_decay), leading(backwards)), reverse=True)
    entering = jnp.moveaxis(entering, 0, 1)
    from_right = jnp.moveaxis(from_right, 0, 1)
    q_adjoint = jnp.exp(cumlog) * (product('hbcv,hbdv->hbcd', o_grad, entering) + product('hbcs,hbsd->hbcd', out_dots, k_shrunk))
    k_grad = jnp.exp(-cumlog) * product('hbcs,hbcd->hbsd', out_dots, q_grown) + k_tail * product('hbsv,hbdv->hbsd', v_heads, from_right)
    v_grad = product('hbcs,hbcv->hbsv', key_dots, o_grad) + product('hbsd,hbdv->hbsv', k_tailed, from_right)
    decay_terms = merge_heads(q_heads * q_adjoint - k_heads * k_grad)
    d_log_decay = jnp.flip(jnp.cumsum(jnp.flip(decay_terms, 0), 0), 0)
    value_grad = merge_heads(v_grad).astype(jnp.bfloat16)
    d_w_value = lax.dot_general(block_input, value_grad, (((0,), (0,)), ((), ())), preferred_element_type=jnp.float32)
    row_norms = jnp.sum(d_w_value * d_w_value, axis=1)
    return (merge_heads(q_adjoint * q_scale).astype(jnp.bfloat16), merge_heads(k_grad).astype(jnp.bfloat16), d_log_decay, d_w_value, row_norms)
```

```python
import jax
import jax.numpy as jnp
from jax import lax
from jax.experimental import pallas as pl
from jax.experimental.pallas import tpu as pltpu
from jax.sharding import PartitionSpec as P

DK = 128
DV = 256
T = 256
BLK = 32
NB = T // BLK
NZ, NX, NT = 8, 4, 8
SLAB = DV // NX
ROWS = 64
MESH = pl.DeviceIdType.MESH
F32, BF16 = jnp.float32, jnp.bfloat16


def dot(a, b):
    return jnp.dot(a, b, preferred_element_type=F32)


def dot_nt(a, b):
    return lax.dot_general(a, b, (((1,), (1,)), ((), ())), preferred_element_type=F32)


def dot_tn(a, b):
    return lax.dot_general(a, b, (((0,), (0,)), ((), ())), preferred_element_type=F32)


def exact_sum(ones, a):
    hi = a.astype(BF16)
    rest = a - hi.astype(F32)
    mid = rest.astype(BF16)
    low = (rest - mid.astype(F32)).astype(BF16)
    return dot(ones, hi) + (dot(ones, mid) + dot(ones, low))


def kernel(
    x_hbm, q_hbm, k_hbm, w_hbm, g_hbm, do_hbm,
    dq_hbm, dk_hbm, dg_hbm, dw_hbm, rn_hbm,
    x_v, q_v, k_v, w_v, g_v, do_v, dq_v, dk_v, dg_v, dwo_v, rn_v,
    xt_v, val_v, locs_v, adjs_v,
    x1s, x1r, z2s, z2r, x3s, x3r, dwp, rxr, rxs, rzr, tps, tpr,
    in_sem, out_sem, x1_ss, x1_rs, z2_ss, z2_rs, x3_ss, x3_rs, rx_ss, rx_rs, rz_ss, rz_rs, tp_ss, tp_rs,
):
    sp, tp = lax.axis_index("sp"), lax.axis_index("tp")
    z, x = sp // NX, lax.rem(sp, NX)

    def x_dev(t):
        return {"sp": z * NX + t}

    def z_dev(t):
        return {"sp": t * NX + x}

    def tp_dev(t):
        return {"tp": t}

    barrier = pltpu.get_barrier_semaphore()
    for k in range(1, NX):
        pl.semaphore_signal(barrier, inc=1, device_id=x_dev(lax.rem(x + k, NX)), device_id_type=MESH)
    for k in range(1, NZ):
        pl.semaphore_signal(barrier, inc=1, device_id=z_dev(lax.rem(z + k, NZ)), device_id_type=MESH)
    for k in range(1, NT):
        pl.semaphore_signal(barrier, inc=1, device_id=tp_dev(lax.rem(tp + k, NT)), device_id_type=MESH)

    loads = [
        pltpu.make_async_copy(src, dst, in_sem.at[i])
        for i, (src, dst) in enumerate(
            ((g_hbm, g_v), (q_hbm, q_v), (do_hbm, do_v), (k_hbm, k_v), (x_hbm, x_v), (w_hbm, w_v))
        )
    ]
    for load in loads:
        load.start()

    def remote(src, dst, ss, rs, dev):
        return pltpu.make_async_remote_copy(
            src_ref=src, dst_ref=dst, send_sem=ss, recv_sem=rs, device_id=dev, device_id_type=MESH
        )

    row = lax.broadcasted_iota(jnp.int32, (T, T), 0)
    col = lax.broadcasted_iota(jnp.int32, (T, T), 1)
    same = (row >> 5) == (col >> 5)
    lower = same & (col <= row)
    upper = same & (col >= row)

    loads[0].wait()
    c = exact_sum(lower.astype(BF16), g_v[...])
    c3 = c.reshape(NB, BLK, DK)
    ends = [c3[b, BLK - 1 : BLK, :] for b in range(NB)]
    before = [jnp.zeros((1, DK), F32)]
    for b in range(NB):
        before.append(before[-1] + ends[b])
    after = [jnp.zeros((1, DK), F32)]
    for b in reversed(range(1, NB)):
        after.append(after[-1] + ends[b])
    after = after[::-1]
    total = before[NB]

    def per_block(rows):
        return jnp.concatenate([jnp.broadcast_to(r, (BLK, DK)) for r in rows], axis=0)

    end_wide = per_block(ends)
    from_start = jnp.exp(c + per_block(before[:NB]))
    tail_log = end_wide - c
    to_end = jnp.exp(tail_log + per_block(after))
    span_decay = jnp.exp(total)

    loads[1].wait()
    loads[2].wait()
    qs = q_v[...].astype(F32) * (DK**-0.5)
    do = do_v[...]
    span_adj = dot_tn(do, (qs * from_start).astype(BF16))
    wide_decay = jnp.broadcast_to(span_decay, (8, DK))
    for s in range(NX):
        x1s[0, s, :SLAB, :] = span_adj[s * SLAB : (s + 1) * SLAB]
        x1s[0, s, SLAB:, :] = wide_decay
    pl.semaphore_wait(barrier, NX - 1 + NZ - 1 + NT - 1)

    started = []

    def x_leg(i):
        for k in (2, 1, 3):
            t = lax.rem(x + k, NX)
            cp = remote(x1s.at[i, t], x1r.at[i, x], x1_ss.at[i, k], x1_rs.at[i, k], x_dev(t))
            cp.start()
            started.append(cp)
        x1r[i, x] = x1s[i, x]

    def x_leg_wait(i):
        for k in (2, 1, 3):
            t = lax.rem(x + NX - k, NX)
            remote(x1s.at[i, t], x1r.at[i, t], x1_ss.at[i, k], x1_rs.at[i, k], x_dev(t)).wait_recv()

    x_leg(0)

    loads[3].wait()
    kf = k_v[...].astype(F32)
    k_end = (kf * to_end).astype(BF16)
    loads[4].wait()
    loads[5].wait()
    val_v[...] = dot(x_v[...], w_v[...]).astype(BF16)
    v = val_v[...]
    span_state = dot_tn(v, k_end)
    for s in range(NX):
        x1s[1, s, :SLAB, :] = span_state[s * SLAB : (s + 1) * SLAB]
        x1s[1, s, SLAB:, :] = wide_decay
    x_leg(1)

    def slab(i, t):
        return x1r[i, t, :SLAB, :]

    def slab_decay(i, t):
        return x1r[i, t, SLAB : SLAB + 1, :]

    def group_total(i, order):
        x_leg_wait(i)
        acc = slab(i, order[0])
        dec = slab_decay(i, order[0])
        for t in order[1:]:
            acc = slab(i, t) + slab_decay(i, t) * acc
            dec = dec * slab_decay(i, t)
        z2s[i, :SLAB, :] = acc
        z2s[i, SLAB:, :] = jnp.broadcast_to(dec, (8, DK))

    def z_copy(i, k, t, slot):
        return remote(z2s.at[i], z2r.at[i, slot], z2_ss.at[i, k], z2_rs.at[i, k], z_dev(t))

    group_total(0, (3, 2, 1, 0))
    for k in (4, 3, 5, 2, 6, 1, 7):
        @pl.when(z >= k)
        def _():
            z_copy(0, k, z - k, z).start()

    group_total(1, (0, 1, 2, 3))
    for k in (4, 3, 5, 2, 6, 1, 7):
        @pl.when(z + k < NZ)
        def _():
            z_copy(1, k, z + k, z).start()

    exp_c = jnp.exp(c)
    exp_nc = jnp.exp(-c)
    exp_tail = jnp.exp(tail_log)
    grown_q = (qs * exp_c).astype(BF16)
    shrunk_k = (kf * exp_nc).astype(BF16)
    tail_k = (kf * exp_tail).astype(BF16)
    adj = jnp.zeros((DV, DK), F32)
    for b in reversed(range(NB)):
        sl = slice(b * BLK, (b + 1) * BLK)
        adjs_v[b] = adj.astype(BF16)
        if b:
            adj = jnp.exp(ends[b]) * adj + dot_tn(do[sl], grown_q[sl])
    key_dots_t = jnp.where(upper, dot_nt(shrunk_k, grown_q), 0.0).astype(BF16)
    local_vg = dot(key_dots_t, do) + jnp.concatenate(
        [dot_nt(tail_k[b * BLK : (b + 1) * BLK], adjs_v[b]) for b in range(NB)], axis=0
    )

    def enter(i, t, acc):
        x3s[i, t] = acc

    def x3_leg(i):
        for k in (2, 1, 3):
            t = lax.rem(x + k, NX)
            cp = remote(x3s.at[i, t], x3r.at[i, x], x3_ss.at[i, k], x3_rs.at[i, k], x_dev(t))
            cp.start()
            started.append(cp)
        x3r[i, x] = x3s[i, x]

    def x3_wait(i):
        for k in (2, 1, 3):
            t = lax.rem(x + NX - k, NX)
            remote(x3s.at[i, t], x3r.at[i, t], x3_ss.at[i, k], x3_rs.at[i, k], x_dev(t)).wait_recv()

    def adj_step(n, acc):
        t = NZ - 1 - n
        z_copy(0, t - z, t, t).wait_recv()
        return z2r[0, t, :SLAB, :] + z2r[0, t, SLAB : SLAB + 1, :] * acc

    acc = lax.fori_loop(0, NZ - 1 - z, adj_step, jnp.zeros((SLAB, DK), F32))
    for t in (3, 2, 1, 0):
        enter(0, t, acc)
        if t:
            acc = slab(0, t) + slab_decay(0, t) * acc
    x3_leg(0)

    def state_step(t, acc):
        z_copy(1, z - t, t, t).wait_recv()
        return z2r[1, t, :SLAB, :] + z2r[1, t, SLAB : SLAB + 1, :] * acc

    acc = lax.fori_loop(0, z, state_step, jnp.zeros((SLAB, DK), F32))
    for t in range(NX):
        enter(1, t, acc)
        if t < NX - 1:
            acc = slab(1, t) + slab_decay(1, t) * acc
    x3_leg(1)

    for zz in range(NZ):
        xt_v[:, zz] = x_v[:, zz * NX * ROWS : (zz + 1) * NX * ROWS].T.reshape(NX, ROWS, T)

    x3_wait(0)
    adj_in = x3r[0].reshape(DV, DK)
    adj_in16 = adj_in.astype(BF16)
    vg = (local_vg + dot_nt(k_end, adj_in16)).astype(BF16)
    for k in (2, 1, 3, 0):
        t = lax.rem(x + k, NX)
        part = dot(xt_v[t].reshape(NZ * ROWS, T), vg)
        for h in range(2):
            dwp[h, t] = part[:, h * 128 : (h + 1) * 128].reshape(NZ, ROWS, 128)
            if k:
                cp = remote(dwp.at[h, t], rxr.at[h, x], rx_ss.at[h, k], rx_rs.at[h, k], x_dev(t))
                cp.start()
                started.append(cp)

    state = jnp.zeros((DV, DK), F32)
    for b in range(NB):
        sl = slice(b * BLK, (b + 1) * BLK)
        locs_v[b] = state.astype(BF16)
        if b < NB - 1:
            state = jnp.exp(ends[b]) * state + dot_tn(v[sl], tail_k[sl])
    out_dots = jnp.where(lower, dot_nt(do, v), 0.0).astype(BF16)
    out_dots_t = jnp.where(upper, dot_nt(v, do), 0.0).astype(BF16)
    local_qg = dot(out_dots, shrunk_k) + jnp.concatenate(
        [dot(do[b * BLK : (b + 1) * BLK], locs_v[b]) for b in range(NB)], axis=0
    )
    local_kg = exp_nc * dot(out_dots_t, grown_q) + exp_tail * jnp.concatenate(
        [dot(v[b * BLK : (b + 1) * BLK], adjs_v[b]) for b in range(NB)], axis=0
    )
    kg = local_kg + to_end * dot(v, adj_in16)
    dk_v[...] = kg.astype(BF16)
    x3_wait(1)
    state_in = x3r[1].reshape(DV, DK)
    qg = exp_c * local_qg + from_start * dot(do, state_in.astype(BF16))
    dq_v[...] = (qg * (DK**-0.5)).astype(BF16)
    carry = jnp.sum(adj_in * (span_state + span_decay * state_in), axis=0, keepdims=True)
    dg_v[...] = exact_sum((col >= row).astype(BF16), qs * qg - kf * kg) + carry
    stores = [
        pltpu.make_async_copy(src, dst, out_sem.at[i])
        for i, (src, dst) in enumerate(((dq_v, dq_hbm), (dk_v, dk_hbm), (dg_v, dg_hbm), (dwo_v, dw_hbm), (rn_v, rn_hbm)))
    ]
    for store in stores[:3]:
        store.start()

    for h in range(2):
        for k in (2, 1, 3):
            t = lax.rem(x + NX - k, NX)
            remote(dwp.at[h, t], rxr.at[h, t], rx_ss.at[h, k], rx_rs.at[h, k], x_dev(t)).wait_recv()
        for k in (4, 3, 5, 2, 6, 1, 7, 0):
            t = lax.rem(z + k, NZ)
            piece = dwp[h, x, t]
            for j in range(1, NX):
                piece = piece + rxr[h, lax.rem(x + j, NX), t]
            rxs[h, t] = piece
            if k:
                cp = remote(rxs.at[h, t], rzr.at[h, z], rz_ss.at[h, k], rz_rs.at[h, k], z_dev(t))
                cp.start()
                started.append(cp)
    squares = jnp.zeros((ROWS, 128), F32)
    for h in range(2):
        piece = rxs[h, z]
        for k in (1, 7, 2, 6, 3, 5, 4):
            t = lax.rem(z + NZ - k, NZ)
            remote(rxs.at[h, t], rzr.at[h, t], rz_ss.at[h, k], rz_rs.at[h, k], z_dev(t)).wait_recv()
            piece = piece + rzr[h, t]
        dwo_v[:, h * 128 : (h + 1) * 128] = piece
        squares = squares + piece * piece
    stores[3].start()

    norms = jnp.sum(squares.T, axis=0, keepdims=True)
    tps[...] = jnp.broadcast_to(jnp.concatenate([norms, jnp.zeros((1, 64), F32)], axis=1), (8, 128))
    for k in range(1, NT):
        t = lax.rem(tp + k, NT)
        cp = remote(tps, tpr.at[tp], tp_ss.at[k], tp_rs.at[k], tp_dev(t))
        cp.start()
        started.append(cp)
    acc = tps[0:1, :]
    for k in range(1, NT):
        t = lax.rem(tp + NT - k, NT)
        remote(tps, tpr.at[t], tp_ss.at[k], tp_rs.at[k], tp_dev(t)).wait_recv()
        acc = acc + tpr[t, 0:1, :]
    rn_v[...] = acc[:, :ROWS]
    stores[4].start()

    for cp in started:
        cp.wait_send()
    for k in range(1, NZ):
        @pl.when(z >= k)
        def _():
            z_copy(0, k, z - k, z).wait_send()

        @pl.when(z + k < NZ)
        def _():
            z_copy(1, k, z + k, z).wait_send()
    for store in stores:
        store.wait()


def on_device(block_input, queries, keys, w_value, log_decay, d_out):
    any_spec = pl.BlockSpec(memory_space=pl.ANY)
    dma = pltpu.SemaphoreType.DMA
    outs = pl.pallas_call(
        kernel,
        out_shape=(
            jax.ShapeDtypeStruct((T, DK), BF16),
            jax.ShapeDtypeStruct((T, DK), BF16),
            jax.ShapeDtypeStruct((T, DK), F32),
            jax.ShapeDtypeStruct((ROWS, DV), F32),
            jax.ShapeDtypeStruct((1, ROWS), F32),
        ),
        in_specs=[any_spec] * 6,
        out_specs=(any_spec,) * 5,
        scratch_shapes=[
            pltpu.VMEM((T, 2048), BF16), pltpu.VMEM((T, DK), BF16), pltpu.VMEM((T, DK), BF16),
            pltpu.VMEM((2048, DV), BF16), pltpu.VMEM((T, DK), F32), pltpu.VMEM((T, DV), BF16),
            pltpu.VMEM((T, DK), BF16), pltpu.VMEM((T, DK), BF16), pltpu.VMEM((T, DK), F32),
            pltpu.VMEM((ROWS, DV), F32), pltpu.VMEM((1, ROWS), F32),
            pltpu.VMEM((NX, NZ, ROWS, T), BF16), pltpu.VMEM((T, DV), BF16),
            pltpu.VMEM((NB, DV, DK), BF16), pltpu.VMEM((NB, DV, DK), BF16),
            pltpu.VMEM((2, NX, SLAB + 8, DK), F32), pltpu.VMEM((2, NX, SLAB + 8, DK), F32),
            pltpu.VMEM((2, SLAB + 8, DK), F32), pltpu.VMEM((2, NZ, SLAB + 8, DK), F32),
            pltpu.VMEM((2, NX, SLAB, DK), F32), pltpu.VMEM((2, NX, SLAB, DK), F32),
            pltpu.VMEM((2, NX, NZ, ROWS, 128), F32), pltpu.VMEM((2, NX, NZ, ROWS, 128), F32),
            pltpu.VMEM((2, NZ, ROWS, 128), F32), pltpu.VMEM((2, NZ, ROWS, 128), F32),
            pltpu.VMEM((8, 128), F32), pltpu.VMEM((NT, 8, 128), F32),
            dma((6,)), dma((5,)), dma((2, NX)), dma((2, NX)), dma((2, NZ)), dma((2, NZ)),
            dma((2, NX)), dma((2, NX)), dma((2, NX)), dma((2, NX)), dma((2, NZ)), dma((2, NZ)),
            dma((NT,)), dma((NT,)),
        ],
        compiler_params=pltpu.CompilerParams(collective_id=0, has_side_effects=True),
        name="gla_backward",
    )(block_input, queries, keys, w_value, log_decay, d_out)
    return (*outs[:4], outs[4].reshape(ROWS))


def solution(mesh):
    in_specs = (P("sp", None), P("sp", "tp"), P("sp", "tp"), P(None, "tp"), P("sp", "tp"), P("sp", "tp"))
    out_specs = (P("sp", "tp"), P("sp", "tp"), P("sp", "tp"), P("sp", "tp"), P("sp"))
    return jax.shard_map(on_device, mesh=mesh, in_specs=in_specs, out_specs=out_specs, check_vma=False)
```

```python
import jax
import jax.numpy as jnp
from jax import lax
from jax.experimental import pallas as pl
from jax.experimental.pallas import tpu as pltpu
from jax.sharding import PartitionSpec as P

DK = 128
DV = 256
T = 256
BLK = 32
NB = T // BLK
NZ, NX, NT = 8, 4, 8
SLAB = DV // NX
ROWS = 64
MESH = pl.DeviceIdType.MESH
F32, BF16 = jnp.float32, jnp.bfloat16


def dot(a, b):
    return jnp.dot(a, b, preferred_element_type=F32)


def dot_nt(a, b):
    return lax.dot_general(a, b, (((1,), (1,)), ((), ())), preferred_element_type=F32)


def dot_tn(a, b):
    return lax.dot_general(a, b, (((0,), (0,)), ((), ())), preferred_element_type=F32)


def exact_sum(ones, a):
    hi = a.astype(BF16)
    rest = a - hi.astype(F32)
    mid = rest.astype(BF16)
    low = (rest - mid.astype(F32)).astype(BF16)
    return dot(ones, hi) + (dot(ones, mid) + dot(ones, low))


def kernel(
    x_hbm, q_hbm, k_hbm, w_hbm, g_hbm, do_hbm,
    dq_hbm, dk_hbm, dg_hbm, dw_hbm, rn_hbm,
    x_v, q_v, k_v, w_v, g_v, do_v, dq_v, dk_v, dg_v, dwo_v, rn_v,
    xt_v, val_v, locs_v, adjs_v, as_v, vgs_v, xb_v,
    x1s, x1r, z2s, z2r, x3s, x3r, gx, xts, xg, dwp, rzr, tps, tpr,
    in_sem, out_sem, x1_ss, x1_rs, z2_ss, z2_rs, x3_ss, x3_rs, gx_ss, gx_rs, xx_ss, xx_rs, xy_ss, xy_rs,
    xc_ss, xc_rs, rz_ss, rz_rs, tp_ss, tp_rs,
):
    sp, tp = lax.axis_index("sp"), lax.axis_index("tp")
    z, x = sp // NX, lax.rem(sp, NX)

    def x_dev(t):
        return {"sp": z * NX + t}

    def z_dev(t):
        return {"sp": t * NX + x}

    def tp_dev(t):
        return {"tp": t}

    barrier = pltpu.get_barrier_semaphore()
    for k in range(1, NX):
        pl.semaphore_signal(barrier, inc=1, device_id=x_dev(lax.rem(x + k, NX)), device_id_type=MESH)
    for k in range(1, NZ):
        pl.semaphore_signal(barrier, inc=1, device_id=z_dev(lax.rem(z + k, NZ)), device_id_type=MESH)
    for k in range(1, NT):
        pl.semaphore_signal(barrier, inc=1, device_id=tp_dev(lax.rem(tp + k, NT)), device_id_type=MESH)

    loads = [
        pltpu.make_async_copy(src, dst, in_sem.at[i])
        for i, (src, dst) in enumerate(
            ((g_hbm, g_v), (q_hbm, q_v), (do_hbm, do_v), (k_hbm, k_v), (x_hbm, x_v), (w_hbm, w_v))
        )
    ]
    for load in loads:
        load.start()

    started = []

    def go(cp):
        cp.start()
        started.append(cp)

    def remote(src, dst, ss, rs, dev):
        return pltpu.make_async_remote_copy(
            src_ref=src, dst_ref=dst, send_sem=ss, recv_sem=rs, device_id=dev, device_id_type=MESH
        )

    row = lax.broadcasted_iota(jnp.int32, (T, T), 0)
    col = lax.broadcasted_iota(jnp.int32, (T, T), 1)
    same = (row >> 5) == (col >> 5)
    lower = same & (col <= row)
    upper = same & (col >= row)

    loads[0].wait()
    c = exact_sum(lower.astype(BF16), g_v[...])
    c3 = c.reshape(NB, BLK, DK)
    ends = [c3[b, BLK - 1 : BLK, :] for b in range(NB)]
    before = [jnp.zeros((1, DK), F32)]
    for b in range(NB):
        before.append(before[-1] + ends[b])
    after = [jnp.zeros((1, DK), F32)]
    for b in reversed(range(1, NB)):
        after.append(after[-1] + ends[b])
    after = after[::-1]
    total = before[NB]

    def per_block(rows):
        return jnp.concatenate([jnp.broadcast_to(r, (BLK, DK)) for r in rows], axis=0)

    end_wide = per_block(ends)
    from_start = jnp.exp(c + per_block(before[:NB]))
    tail_log = end_wide - c
    to_end = jnp.exp(tail_log + per_block(after))
    span_decay = jnp.exp(total)

    loads[1].wait()
    loads[2].wait()
    qs = q_v[...].astype(F32) * (DK**-0.5)
    do = do_v[...]
    span_adj = dot_tn(do, (qs * from_start).astype(BF16))
    wide_decay = jnp.broadcast_to(span_decay, (8, DK))
    for s in range(NX):
        x1s[0, s, :SLAB, :] = span_adj[s * SLAB : (s + 1) * SLAB]
        x1s[0, s, SLAB:, :] = wide_decay

    loads[3].wait()
    kf = k_v[...].astype(F32)
    exp_c = jnp.exp(c)
    exp_nc = jnp.exp(-c)
    exp_tail = jnp.exp(tail_log)
    grown_q = (qs * exp_c).astype(BF16)
    shrunk_k = (kf * exp_nc).astype(BF16)
    tail_k = (kf * exp_tail).astype(BF16)
    k_end = kf * to_end
    adj = jnp.zeros((DV, DK), F32)
    for b in reversed(range(NB)):
        sl = slice(b * BLK, (b + 1) * BLK)
        adjs_v[b] = adj.astype(BF16)
        if b:
            adj = jnp.exp(ends[b]) * adj + dot_tn(do[sl], grown_q[sl])
    key_dots_t = jnp.where(upper, dot_nt(shrunk_k, grown_q), 0.0).astype(BF16)
    local_vg = dot(key_dots_t, do) + jnp.concatenate(
        [dot_nt(tail_k[b * BLK : (b + 1) * BLK], adjs_v[b]) for b in range(NB)], axis=0
    )
    gx[x, 0] = local_vg[:, :DK]
    gx[x, 1] = local_vg[:, DK:]
    gx[x, 2] = k_end
    gx[x, 3] = span_adj

    loads[4].wait()
    for zz in range(NZ):
        xt_v[:, zz] = x_v[:, zz * NX * ROWS : (zz + 1) * NX * ROWS].T.reshape(NX, ROWS, T)
    for t in range(NX):
        xts[t] = xt_v[t, tp].astype(F32)
    pl.semaphore_wait(barrier, NX - 1 + NZ - 1 + NT - 1)

    def x1_copy(i, k, src, slot, to):
        return remote(x1s.at[i, src], x1r.at[i, slot], x1_ss.at[i, k], x1_rs.at[i, k], x_dev(to))

    def x_leg(i):
        for k in (2, 1, 3):
            t = lax.rem(x + k, NX)
            go(x1_copy(i, k, t, x, t))
        x1r[i, x] = x1s[i, x]

    def x_leg_wait(i):
        for k in (2, 1, 3):
            t = lax.rem(x + NX - k, NX)
            x1_copy(i, k, t, t, t).wait_recv()

    x_leg(0)

    def xx_copy(k, t):
        return remote(xts.at[t], xg.at[tp, 3 - k], xx_ss.at[k], xx_rs.at[k], x_dev(t))

    for k in (2, 1, 3):
        go(xx_copy(k, lax.rem(x + k, NX)))

    right, left, far = lax.rem(x + 1, NX), lax.rem(x + 3, NX), lax.rem(x + 2, NX)

    def gx_copy(n, slot, part, to):
        ref = gx.at[slot, pl.ds(part, 2)]
        return remote(ref, ref, gx_ss.at[n], gx_rs.at[n], x_dev(to))

    go(gx_copy(0, x, 0, right))
    go(gx_copy(1, x, 2, left))
    go(gx_copy(2, x, 2, right))
    go(gx_copy(3, x, 0, left))

    loads[5].wait()
    val_v[...] = dot(x_v[...], w_v[...]).astype(BF16)
    v = val_v[...]
    span_state = dot_tn(v, k_end.astype(BF16))
    for s in range(NX):
        x1s[1, s, :SLAB, :] = span_state[s * SLAB : (s + 1) * SLAB]
        x1s[1, s, SLAB:, :] = wide_decay
    x_leg(1)

    def slab(i, t):
        return x1r[i, t, :SLAB, :]

    def slab_decay(i, t):
        return x1r[i, t, SLAB : SLAB + 1, :]

    def group_total(i, order):
        x_leg_wait(i)
        acc = slab(i, order[0])
        dec = slab_decay(i, order[0])
        for t in order[1:]:
            acc = slab(i, t) + slab_decay(i, t) * acc
            dec = dec * slab_decay(i, t)
        z2s[i, :SLAB, :] = acc
        z2s[i, SLAB:, :] = jnp.broadcast_to(dec, (8, DK))

    def z_copy(i, k, t, slot):
        return remote(z2s.at[i], z2r.at[i, slot], z2_ss.at[i, k], z2_rs.at[i, k], z_dev(t))

    group_total(0, (3, 2, 1, 0))
    for k in (4, 3, 5, 2, 6, 1, 7):
        @pl.when(z >= k)
        def _():
            z_copy(0, k, z - k, z).start()

    sibling = tp + 1 - 2 * lax.rem(tp, 2)

    def xy_copy(j, slot, to):
        return remote(xg.at[slot], xg.at[slot], xy_ss.at[j], xy_rs.at[j], tp_dev(to))

    def xc_copy(j, slot):
        return remote(xg.at[slot], xg.at[slot], xc_ss.at[j], xc_rs.at[j], tp_dev(sibling))

    for k in (1, 3, 2):
        xx_copy(k, lax.rem(x + NX - k, NX)).wait_recv()
    for j in (2, 1, 3):
        go(xy_copy(j, tp, lax.rem(tp + 2 * j, NT)))
    go(xc_copy(0, tp))

    gx_copy(0, left, 0, right).wait_recv()
    go(gx_copy(4, left, 0, right))
    gx_copy(1, right, 2, left).wait_recv()
    go(gx_copy(5, right, 2, left))

    def adj_step(n, acc):
        t = NZ - 1 - n
        z_copy(0, t - z, t, t).wait_recv()
        return z2r[0, t, :SLAB, :] + z2r[0, t, SLAB : SLAB + 1, :] * acc

    x3s[0, 0] = lax.fori_loop(0, NZ - 1 - z, adj_step, jnp.zeros((SLAB, DK), F32))

    def x3_copy(i, k, src, slot, to):
        return remote(x3s.at[i, src], x3r.at[i, slot], x3_ss.at[i, k], x3_rs.at[i, k], x_dev(to))

    def x3_wait(i):
        for k in (2, 1, 3):
            t = lax.rem(x + NX - k, NX)
            x3_copy(i, k, 0, t, t).wait_recv()

    for k in (2, 1, 3):
        go(x3_copy(0, k, 0, x, lax.rem(x + k, NX)))
    x3r[0, x] = x3s[0, 0]

    group_total(1, (0, 1, 2, 3))
    for k in (4, 3, 5, 2, 6, 1, 7):
        @pl.when(z + k < NZ)
        def _():
            z_copy(1, k, z + k, z).start()

    for j in (1, 3, 2):
        slot = lax.rem(tp + NT - 2 * j, NT)
        xy_copy(j, slot, slot).wait_recv()
        go(xc_copy(j, slot))
    for j in (0, 1, 3, 2):
        xc_copy(j, lax.rem(sibling + NT - 2 * j, NT)).wait_recv()

    def columns(t):
        return pl.ds(pl.multiple_of(t * T, T), T)

    xb_v[:, :, columns(x)] = xt_v[x]
    for k in range(1, NX):
        xb_v[:, :, columns(lax.rem(x + k, NX))] = xg[:, k - 1].astype(BF16)

    gx_copy(2, left, 2, left).wait_recv()
    gx_copy(3, right, 0, right).wait_recv()
    gx_copy(4, far, 0, left).wait_recv()
    gx_copy(5, far, 2, right).wait_recv()
    x3_wait(0)

    acc = x3r[0].reshape(DV, DK)
    for t in (3, 2, 1, 0):
        as_v[t] = acc
        k_t = gx[t, 2].astype(BF16)
        acc16 = acc.astype(BF16)
        for h in range(2):
            hl = slice(h * DK, (h + 1) * DK)
            vgs_v[t * T : (t + 1) * T, hl] = (gx[t, h] + dot_nt(k_t, acc16[hl])).astype(BF16)
        if t:
            acc = gx[t, 3] + slab_decay(0, t) * acc
    dwp[...] = dot(xb_v[...].reshape(NZ * ROWS, NX * T), vgs_v[...]).reshape(NZ, ROWS, DV)

    def rz_copy(k, src, slot, to):
        return remote(dwp.at[src], rzr.at[slot], rz_ss.at[k], rz_rs.at[k], z_dev(to))

    for k in (4, 3, 5, 2, 6, 1, 7):
        t = lax.rem(z + k, NZ)
        go(rz_copy(k, t, z, t))
    adj_in = as_v[x]
    adj_in16 = adj_in.astype(BF16)

    state = jnp.zeros((DV, DK), F32)
    for b in range(NB):
        sl = slice(b * BLK, (b + 1) * BLK)
        locs_v[b] = state.astype(BF16)
        if b < NB - 1:
            state = jnp.exp(ends[b]) * state + dot_tn(v[sl], tail_k[sl])
    out_dots = jnp.where(lower, dot_nt(do, v), 0.0).astype(BF16)
    out_dots_t = jnp.where(upper, dot_nt(v, do), 0.0).astype(BF16)
    local_qg = dot(out_dots, shrunk_k) + jnp.concatenate(
        [dot(do[b * BLK : (b + 1) * BLK], locs_v[b]) for b in range(NB)], axis=0
    )
    local_kg = exp_nc * dot(out_dots_t, grown_q) + exp_tail * jnp.concatenate(
        [dot(v[b * BLK : (b + 1) * BLK], adjs_v[b]) for b in range(NB)], axis=0
    )
    kg = local_kg + to_end * dot(v, adj_in16)
    dk_v[...] = kg.astype(BF16)

    def state_step(t, acc):
        z_copy(1, z - t, t, t).wait_recv()
        return z2r[1, t, :SLAB, :] + z2r[1, t, SLAB : SLAB + 1, :] * acc

    acc = lax.fori_loop(0, z, state_step, jnp.zeros((SLAB, DK), F32))
    for t in range(NX):
        x3s[1, t] = acc
        if t < NX - 1:
            acc = slab(1, t) + slab_decay(1, t) * acc
    for k in (2, 1, 3):
        t = lax.rem(x + k, NX)
        go(x3_copy(1, k, t, x, t))
    x3r[1, x] = x3s[1, x]
    x3_wait(1)
    state_in = x3r[1].reshape(DV, DK)
    qg = exp_c * local_qg + from_start * dot(do, state_in.astype(BF16))
    dq_v[...] = (qg * (DK**-0.5)).astype(BF16)
    carry = jnp.sum(adj_in * (span_state + span_decay * state_in), axis=0, keepdims=True)
    dg_v[...] = exact_sum((col >= row).astype(BF16), qs * qg - kf * kg) + carry
    stores = [
        pltpu.make_async_copy(src, dst, out_sem.at[i])
        for i, (src, dst) in enumerate(((dq_v, dq_hbm), (dk_v, dk_hbm), (dg_v, dg_hbm), (dwo_v, dw_hbm), (rn_v, rn_hbm)))
    ]
    for store in stores[:3]:
        store.start()

    total_dw = dwp[z]
    for k in (1, 7, 2, 6, 3, 5, 4):
        t = lax.rem(z + NZ - k, NZ)
        rz_copy(k, t, t, t).wait_recv()
        total_dw = total_dw + rzr[t]
    dwo_v[...] = total_dw
    stores[3].start()

    squares = total_dw[:, :DK] * total_dw[:, :DK] + total_dw[:, DK:] * total_dw[:, DK:]
    norms = jnp.sum(squares.T, axis=0, keepdims=True)
    tps[...] = jnp.broadcast_to(jnp.concatenate([norms, jnp.zeros((1, 64), F32)], axis=1), (8, 128))

    def tp_copy(k, slot, to):
        return remote(tps, tpr.at[slot], tp_ss.at[k], tp_rs.at[k], tp_dev(to))

    for k in range(1, NT):
        go(tp_copy(k, tp, lax.rem(tp + k, NT)))
    acc = tps[0:1, :]
    for k in range(1, NT):
        t = lax.rem(tp + NT - k, NT)
        tp_copy(k, t, t).wait_recv()
        acc = acc + tpr[t, 0:1, :]
    rn_v[...] = acc[:, :ROWS]
    stores[4].start()

    for cp in started:
        cp.wait_send()
    for k in range(1, NZ):
        @pl.when(z >= k)
        def _():
            z_copy(0, k, z - k, z).wait_send()

        @pl.when(z + k < NZ)
        def _():
            z_copy(1, k, z + k, z).wait_send()
    for store in stores:
        store.wait()


def on_device(block_input, queries, keys, w_value, log_decay, d_out):
    any_spec = pl.BlockSpec(memory_space=pl.ANY)
    dma, vmem = pltpu.SemaphoreType.DMA, pltpu.VMEM
    outs = pl.pallas_call(
        kernel,
        out_shape=(
            jax.ShapeDtypeStruct((T, DK), BF16),
            jax.ShapeDtypeStruct((T, DK), BF16),
            jax.ShapeDtypeStruct((T, DK), F32),
            jax.ShapeDtypeStruct((ROWS, DV), F32),
            jax.ShapeDtypeStruct((1, ROWS), F32),
        ),
        in_specs=[any_spec] * 6,
        out_specs=(any_spec,) * 5,
        scratch_shapes=[
            vmem((T, 2048), BF16), vmem((T, DK), BF16), vmem((T, DK), BF16),
            vmem((2048, DV), BF16), vmem((T, DK), F32), vmem((T, DV), BF16),
            vmem((T, DK), BF16), vmem((T, DK), BF16), vmem((T, DK), F32),
            vmem((ROWS, DV), F32), vmem((1, ROWS), F32),
            vmem((NX, NZ, ROWS, T), BF16), vmem((T, DV), BF16),
            vmem((NB, DV, DK), BF16), vmem((NB, DV, DK), BF16),
            vmem((NX, DV, DK), F32), vmem((NX * T, DV), BF16), vmem((NZ, ROWS, NX * T), BF16),
            vmem((2, NX, SLAB + 8, DK), F32), vmem((2, NX, SLAB + 8, DK), F32),
            vmem((2, SLAB + 8, DK), F32), vmem((2, NZ, SLAB + 8, DK), F32),
            vmem((2, NX, SLAB, DK), F32), vmem((2, NX, SLAB, DK), F32),
            vmem((NX, 4, T, DK), F32), vmem((NX, ROWS, T), F32), vmem((NT, NX - 1, ROWS, T), F32),
            vmem((NZ, ROWS, DV), F32), vmem((NZ, ROWS, DV), F32),
            vmem((8, 128), F32), vmem((NT, 8, 128), F32),
            dma((6,)), dma((5,)), dma((2, NX)), dma((2, NX)), dma((2, NZ)), dma((2, NZ)),
            dma((2, NX)), dma((2, NX)), dma((6,)), dma((6,)), dma((NX,)), dma((NX,)), dma((NX,)), dma((NX,)),
            dma((NX,)), dma((NX,)), dma((NZ,)), dma((NZ,)), dma((NT,)), dma((NT,)),
        ],
        compiler_params=pltpu.CompilerParams(collective_id=0, has_side_effects=True),
        name="gla_backward",
    )(block_input, queries, keys, w_value, log_decay, d_out)
    return (*outs[:4], outs[4].reshape(ROWS))


def solution(mesh):
    in_specs = (P("sp", None), P("sp", "tp"), P("sp", "tp"), P(None, "tp"), P("sp", "tp"), P("sp", "tp"))
    out_specs = (P("sp", "tp"), P("sp", "tp"), P("sp", "tp"), P("sp", "tp"), P("sp"))
    return jax.shard_map(on_device, mesh=mesh, in_specs=in_specs, out_specs=out_specs, check_vma=False)
```

```python
import jax
import jax.numpy as jnp
from jax import lax
from jax.experimental import pallas as pl
from jax.experimental.pallas import tpu as pltpu
from jax.sharding import PartitionSpec as P

DK = 128
DV = 256
T = 256
BLK = 32
NB = T // BLK
NZ, NX, NT = 8, 4, 8
SLAB = DV // NX
ROWS = 64
MESH = pl.DeviceIdType.MESH
F32, BF16 = jnp.float32, jnp.bfloat16


def dot(a, b):
    return jnp.dot(a, b, preferred_element_type=F32)


def dot_nt(a, b):
    return lax.dot_general(a, b, (((1,), (1,)), ((), ())), preferred_element_type=F32)


def dot_tn(a, b):
    return lax.dot_general(a, b, (((0,), (0,)), ((), ())), preferred_element_type=F32)


def exact_sum(ones, a):
    hi = a.astype(BF16)
    rest = a - hi.astype(F32)
    mid = rest.astype(BF16)
    low = (rest - mid.astype(F32)).astype(BF16)
    return dot(ones, hi) + (dot(ones, mid) + dot(ones, low))


def kernel(
    x_hbm, q_hbm, k_hbm, w_hbm, g_hbm, do_hbm,
    dq_v, dk_v, dg_v, dwo_v, rn_v,
    x_v, q_v, k_v, w_v, g_v, do_v,
    xt_v, val_v, locs_v, adjs_v, as_v, vgs_v, xb_v,
    x1s, x1r, z2s, z2r, xis, xir, x3s, x3r, gx, xts, xg, dwp, rzr, tps, tpr,
    in_sem, x1_ss, x1_rs, z2_ss, z2_rs, xi_ss, xi_rs, x3_ss, x3_rs, gx_ss, gx_rs, xx_ss, xx_rs, xy_ss, xy_rs,
    xc_ss, xc_rs, rz_ss, rz_rs, tp_ss, tp_rs,
):
    sp, tp = lax.axis_index("sp"), lax.axis_index("tp")
    z, x = sp // NX, lax.rem(sp, NX)

    def x_dev(t):
        return {"sp": z * NX + t}

    def z_dev(t):
        return {"sp": t * NX + x}

    def tp_dev(t):
        return {"tp": t}

    barrier = pltpu.get_barrier_semaphore()
    for k in range(1, NX):
        pl.semaphore_signal(barrier, inc=1, device_id=x_dev(lax.rem(x + k, NX)), device_id_type=MESH)
    for k in range(1, NZ):
        pl.semaphore_signal(barrier, inc=1, device_id=z_dev(lax.rem(z + k, NZ)), device_id_type=MESH)
    for k in range(1, NT):
        pl.semaphore_signal(barrier, inc=1, device_id=tp_dev(lax.rem(tp + k, NT)), device_id_type=MESH)

    loads = [
        pltpu.make_async_copy(src, dst, in_sem.at[i])
        for i, (src, dst) in enumerate(
            ((g_hbm, g_v), (q_hbm, q_v), (do_hbm, do_v), (k_hbm, k_v), (x_hbm, x_v), (w_hbm, w_v))
        )
    ]
    for load in loads:
        load.start()

    started = []

    def go(cp):
        cp.start()
        started.append(cp)

    def remote(src, dst, ss, rs, dev):
        return pltpu.make_async_remote_copy(
            src_ref=src, dst_ref=dst, send_sem=ss, recv_sem=rs, device_id=dev, device_id_type=MESH
        )

    row = lax.broadcasted_iota(jnp.int32, (T, T), 0)
    col = lax.broadcasted_iota(jnp.int32, (T, T), 1)
    same = (row >> 5) == (col >> 5)
    lower = same & (col <= row)
    upper = same & (col >= row)

    loads[0].wait()
    c = exact_sum(lower.astype(BF16), g_v[...])
    c3 = c.reshape(NB, BLK, DK)
    ends = [c3[b, BLK - 1 : BLK, :] for b in range(NB)]
    before = [jnp.zeros((1, DK), F32)]
    for b in range(NB):
        before.append(before[-1] + ends[b])
    after = [jnp.zeros((1, DK), F32)]
    for b in reversed(range(1, NB)):
        after.append(after[-1] + ends[b])
    after = after[::-1]
    total = before[NB]

    def per_block(rows):
        return jnp.concatenate([jnp.broadcast_to(r, (BLK, DK)) for r in rows], axis=0)

    end_wide = per_block(ends)
    from_start = jnp.exp(c + per_block(before[:NB]))
    tail_log = end_wide - c
    to_end = jnp.exp(tail_log + per_block(after))
    span_decay = jnp.exp(total)

    loads[1].wait()
    loads[2].wait()
    qs = q_v[...].astype(F32) * (DK**-0.5)
    do = do_v[...]
    span_adj = dot_tn(do, (qs * from_start).astype(BF16))
    wide_decay = jnp.broadcast_to(span_decay, (8, DK))
    for s in range(NX):
        x1s[0, s, :SLAB, :] = span_adj[s * SLAB : (s + 1) * SLAB]
        x1s[0, s, SLAB:, :] = wide_decay

    loads[3].wait()
    kf = k_v[...].astype(F32)
    exp_c = jnp.exp(c)
    exp_nc = jnp.exp(-c)
    exp_tail = jnp.exp(tail_log)
    grown_q = (qs * exp_c).astype(BF16)
    shrunk_k = (kf * exp_nc).astype(BF16)
    tail_k = (kf * exp_tail).astype(BF16)
    k_end = kf * to_end
    adj = jnp.zeros((DV, DK), F32)
    for b in reversed(range(NB)):
        sl = slice(b * BLK, (b + 1) * BLK)
        adjs_v[b] = adj.astype(BF16)
        if b:
            adj = jnp.exp(ends[b]) * adj + dot_tn(do[sl], grown_q[sl])
    key_dots_t = jnp.where(upper, dot_nt(shrunk_k, grown_q), 0.0).astype(BF16)
    local_vg = dot(key_dots_t, do) + jnp.concatenate(
        [dot_nt(tail_k[b * BLK : (b + 1) * BLK], adjs_v[b]) for b in range(NB)], axis=0
    )
    gx[x, 4] = k_end[: T // 2]
    gx[x, 5] = k_end[T // 2 :]

    loads[4].wait()
    for zz in range(NZ):
        xt_v[:, zz] = x_v[:, zz * NX * ROWS : (zz + 1) * NX * ROWS].T.reshape(NX, ROWS, T)
    for t in range(NX):
        xts[t] = xt_v[t, tp].astype(F32)
    pl.semaphore_wait(barrier, NX - 1 + NZ - 1 + NT - 1)

    def x1_copy(i, k, src, slot, to):
        return remote(x1s.at[i, src], x1r.at[i, slot], x1_ss.at[i, k], x1_rs.at[i, k], x_dev(to))

    def x_leg(i):
        for k in (2, 1, 3):
            t = lax.rem(x + k, NX)
            go(x1_copy(i, k, t, x, t))
        x1r[i, x] = x1s[i, x]

    def x_leg_wait(i):
        for k in (2, 1, 3):
            t = lax.rem(x + NX - k, NX)
            x1_copy(i, k, t, t, t).wait_recv()

    x_leg(0)

    def xx_copy(k, t):
        return remote(xts.at[t], xg.at[tp, 3 - k], xx_ss.at[k], xx_rs.at[k], x_dev(t))

    for k in (2, 1, 3):
        go(xx_copy(k, lax.rem(x + k, NX)))

    right, left, far = lax.rem(x + 1, NX), lax.rem(x + 3, NX), lax.rem(x + 2, NX)
    ways = (right, left, right, left)

    def gx_copy(kind, piece, slot):
        ref = gx.at[slot, piece]
        return remote(ref, ref, gx_ss.at[kind, piece], gx_rs.at[kind, piece], x_dev(ways[kind]))

    def gx_own(first, second):
        for a, b in zip(first + second, second + first):
            go(gx_copy(0, a, x))
            go(gx_copy(1, b, x))

    def gx_forward(first, second):
        for a, b in zip(first, second):
            gx_copy(0, a, left).wait_recv()
            go(gx_copy(2, a, left))
            gx_copy(1, b, right).wait_recv()
            go(gx_copy(3, b, right))

    def gx_wait(first, second):
        for a, b in zip(first, second):
            gx_copy(0, b, left).wait_recv()
            gx_copy(1, a, right).wait_recv()
            gx_copy(2, a, far).wait_recv()
            gx_copy(3, b, far).wait_recv()

    loads[5].wait()
    val_v[...] = dot(x_v[...], w_v[...]).astype(BF16)
    v = val_v[...]
    span_state = dot_tn(v, k_end.astype(BF16))
    for s in range(NX):
        x1s[1, s, :SLAB, :] = span_state[s * SLAB : (s + 1) * SLAB]
        x1s[1, s, SLAB:, :] = wide_decay
    x_leg(1)

    def slab(i, t):
        return x1r[i, t, :SLAB, :]

    def slab_decay(i, t):
        return x1r[i, t, SLAB : SLAB + 1, :]

    def z_copy(i, k, t, slot):
        return remote(z2s.at[i], z2r.at[i, slot], z2_ss.at[i, k], z2_rs.at[i, k], z_dev(t))

    x_leg_wait(0)
    inner = [None] * NX
    inner[3] = jnp.zeros((SLAB, DK), F32)
    for t in (2, 1, 0):
        inner[t] = slab(0, t + 1) + slab_decay(0, t + 1) * inner[t + 1]
    row_decay = slab_decay(0, 0) * slab_decay(0, 1) * slab_decay(0, 2) * slab_decay(0, 3)
    z2s[0, :SLAB, :] = slab(0, 0) + slab_decay(0, 0) * inner[0]
    z2s[0, SLAB:, :] = jnp.broadcast_to(row_decay, (8, DK))
    for k in (4, 3, 5, 2, 6, 1, 7):
        @pl.when(z >= k)
        def _():
            z_copy(0, k, z - k, z).start()

    def xi_copy(k, src, slot, to):
        return remote(xis.at[src], xir.at[slot], xi_ss.at[k], xi_rs.at[k], x_dev(to))

    for t in range(NX):
        xis[t] = inner[t]
    for k in (2, 1, 3):
        t = lax.rem(x + k, NX)
        go(xi_copy(k, t, x, t))
    xir[x] = xis[x]
    gx_own((4,), (5,))

    sibling = tp + 1 - 2 * lax.rem(tp, 2)

    def xy_copy(j, slot, to):
        return remote(xg.at[slot], xg.at[slot], xy_ss.at[j], xy_rs.at[j], tp_dev(to))

    def xc_copy(j, slot):
        return remote(xg.at[slot], xg.at[slot], xc_ss.at[j], xc_rs.at[j], tp_dev(sibling))

    for k in (1, 3, 2):
        xx_copy(k, lax.rem(x + NX - k, NX)).wait_recv()
    for j in (2, 1, 3):
        go(xy_copy(j, tp, lax.rem(tp + 2 * j, NT)))
    go(xc_copy(0, tp))

    for k in (2, 1, 3):
        t = lax.rem(x + NX - k, NX)
        xi_copy(k, t, t, t).wait_recv()
    adj_row = xir[...].reshape(DV, DK)
    row_vg = local_vg + dot_nt(k_end.astype(BF16), adj_row.astype(BF16))
    for h in range(2):
        for p in range(2):
            gx[x, 2 * h + p] = row_vg[p * 128 : (p + 1) * 128, h * DK : (h + 1) * DK]
    gx_own((0, 1), (2, 3))
    gx_forward((4,), (5,))

    def adj_step(n, acc):
        t = NZ - 1 - n
        z_copy(0, t - z, t, t).wait_recv()
        return z2r[0, t, :SLAB, :] + z2r[0, t, SLAB : SLAB + 1, :] * acc

    x3s[0, 0] = lax.fori_loop(0, NZ - 1 - z, adj_step, jnp.zeros((SLAB, DK), F32))

    def x3_copy(i, k, src, slot, to):
        return remote(x3s.at[i, src], x3r.at[i, slot], x3_ss.at[i, k], x3_rs.at[i, k], x_dev(to))

    def x3_wait(i):
        for k in (2, 1, 3):
            t = lax.rem(x + NX - k, NX)
            x3_copy(i, k, 0, t, t).wait_recv()

    for k in (2, 1, 3):
        go(x3_copy(0, k, 0, x, lax.rem(x + k, NX)))
    x3r[0, x] = x3s[0, 0]

    gx_forward((0, 1), (2, 3))
    x_leg_wait(1)
    acc = slab(1, 0)
    for t in range(1, NX):
        acc = slab(1, t) + slab_decay(1, t) * acc
    z2s[1, :SLAB, :] = acc
    z2s[1, SLAB:, :] = jnp.broadcast_to(row_decay, (8, DK))
    for k in (4, 3, 5, 2, 6, 1, 7):
        @pl.when(z + k < NZ)
        def _():
            z_copy(1, k, z + k, z).start()

    for j in (1, 3, 2):
        slot = lax.rem(tp + NT - 2 * j, NT)
        xy_copy(j, slot, slot).wait_recv()
        go(xc_copy(j, slot))
    for j in (0, 1, 3, 2):
        xc_copy(j, lax.rem(sibling + NT - 2 * j, NT)).wait_recv()

    def columns(t):
        return pl.ds(pl.multiple_of(t * T, T), T)

    xb_v[:, :, columns(x)] = xt_v[x]
    for k in range(1, NX):
        xb_v[:, :, columns(lax.rem(x + k, NX))] = xg[:, k - 1].astype(BF16)

    gx_wait((4,), (5,))
    gx_wait((0, 1), (2, 3))
    x3_wait(0)

    acc = x3r[0].reshape(DV, DK)
    for t in (3, 2, 1, 0):
        as_v[t] = acc
        k_t = gx[t, 4:6].reshape(T, DK).astype(BF16)
        acc16 = acc.astype(BF16)
        for h in range(2):
            hl = slice(h * DK, (h + 1) * DK)
            vgs_v[t * T : (t + 1) * T, hl] = (gx[t, 2 * h : 2 * h + 2].reshape(T, DK) + dot_nt(k_t, acc16[hl])).astype(BF16)
        if t:
            acc = slab_decay(0, t) * acc
    dwp[...] = dot(xb_v[...].reshape(NZ * ROWS, NX * T), vgs_v[...]).reshape(NZ, ROWS, DV)

    def rz_copy(k, src, slot, to):
        return remote(dwp.at[src], rzr.at[slot], rz_ss.at[k], rz_rs.at[k], z_dev(to))

    late = []
    for k in (4, 3, 5, 2, 6, 1, 7):
        t = lax.rem(z + k, NZ)
        late.append(rz_copy(k, t, z, t))
        late[-1].start()
    adj_in = adj_row + as_v[x]
    adj_in16 = adj_in.astype(BF16)

    state = jnp.zeros((DV, DK), F32)
    for b in range(NB):
        sl = slice(b * BLK, (b + 1) * BLK)
        locs_v[b] = state.astype(BF16)
        if b < NB - 1:
            state = jnp.exp(ends[b]) * state + dot_tn(v[sl], tail_k[sl])
    out_dots = jnp.where(lower, dot_nt(do, v), 0.0).astype(BF16)
    out_dots_t = jnp.where(upper, dot_nt(v, do), 0.0).astype(BF16)
    local_qg = dot(out_dots, shrunk_k) + jnp.concatenate(
        [dot(do[b * BLK : (b + 1) * BLK], locs_v[b]) for b in range(NB)], axis=0
    )
    local_kg = exp_nc * dot(out_dots_t, grown_q) + exp_tail * jnp.concatenate(
        [dot(v[b * BLK : (b + 1) * BLK], adjs_v[b]) for b in range(NB)], axis=0
    )
    kg = local_kg + to_end * dot(v, adj_in16)
    dk_v[...] = kg.astype(BF16)

    def state_step(t, acc):
        z_copy(1, z - t, t, t).wait_recv()
        return z2r[1, t, :SLAB, :] + z2r[1, t, SLAB : SLAB + 1, :] * acc

    acc = lax.fori_loop(0, z, state_step, jnp.zeros((SLAB, DK), F32))
    for t in range(NX):
        x3s[1, t] = acc
        if t < NX - 1:
            acc = slab(1, t) + slab_decay(1, t) * acc
    for k in (2, 1, 3):
        t = lax.rem(x + k, NX)
        go(x3_copy(1, k, t, x, t))
    x3r[1, x] = x3s[1, x]
    x3_wait(1)
    state_in = x3r[1].reshape(DV, DK)
    qg = exp_c * local_qg + from_start * dot(do, state_in.astype(BF16))
    dq_v[...] = (qg * (DK**-0.5)).astype(BF16)
    carry = jnp.sum(adj_in * (span_state + span_decay * state_in), axis=0, keepdims=True)
    dg_v[...] = exact_sum((col >= row).astype(BF16), qs * qg - kf * kg) + carry
    for cp in started:
        cp.wait_send()
    for k in range(1, NZ):
        @pl.when(z >= k)
        def _():
            z_copy(0, k, z - k, z).wait_send()

        @pl.when(z + k < NZ)
        def _():
            z_copy(1, k, z + k, z).wait_send()

    total_dw = dwp[z]
    for k in (1, 7, 2, 6, 3, 5, 4):
        t = lax.rem(z + NZ - k, NZ)
        rz_copy(k, t, t, t).wait_recv()
        total_dw = total_dw + rzr[t]
    dwo_v[...] = total_dw

    squares = total_dw[:, :DK] * total_dw[:, :DK] + total_dw[:, DK:] * total_dw[:, DK:]
    norms = jnp.sum(squares.T, axis=0, keepdims=True)
    tps[...] = jnp.broadcast_to(jnp.concatenate([norms, jnp.zeros((1, 64), F32)], axis=1), (8, 128))

    def tp_copy(k, slot, to):
        return remote(tps, tpr.at[slot], tp_ss.at[k], tp_rs.at[k], tp_dev(to))

    for k in range(1, NT):
        late.append(tp_copy(k, tp, lax.rem(tp + k, NT)))
        late[-1].start()
    acc = tps[0:1, :]
    for k in range(1, NT):
        t = lax.rem(tp + NT - k, NT)
        tp_copy(k, t, t).wait_recv()
        acc = acc + tpr[t, 0:1, :]
    rn_v[...] = acc[:, :ROWS]
    for cp in late:
        cp.wait_send()


def finish(*refs):
    ins, outs, sem = refs[:5], refs[5:10], refs[10]
    copies = [pltpu.make_async_copy(src, dst, sem.at[i]) for i, (src, dst) in enumerate(zip(ins, outs))]
    for cp in copies:
        cp.start()
    for cp in copies:
        cp.wait()


def on_device(block_input, queries, keys, w_value, log_decay, d_out):
    dma, vmem = pltpu.SemaphoreType.DMA, pltpu.VMEM
    hbm_spec, vmem_spec = pl.BlockSpec(memory_space=pltpu.HBM), pl.BlockSpec(memory_space=vmem)
    shapes = (((T, DK), BF16), ((T, DK), BF16), ((T, DK), F32), ((ROWS, DV), F32), ((1, ROWS), F32))
    args = [
        pltpu.with_memory_space_constraint(a, pltpu.HBM)
        for a in (block_input, queries, keys, w_value, log_decay, d_out)
    ]
    outs = pl.pallas_call(
        kernel,
        out_shape=tuple(vmem(*s) for s in shapes),
        in_specs=[hbm_spec] * 6,
        out_specs=(vmem_spec,) * 5,
        scratch_shapes=[
            vmem((T, 2048), BF16), vmem((T, DK), BF16), vmem((T, DK), BF16),
            vmem((2048, DV), BF16), vmem((T, DK), F32), vmem((T, DV), BF16),
            vmem((NX, NZ, ROWS, T), BF16), vmem((T, DV), BF16),
            vmem((NB, DV, DK), BF16), vmem((NB, DV, DK), BF16),
            vmem((NX, DV, DK), F32), vmem((NX * T, DV), BF16), vmem((NZ, ROWS, NX * T), BF16),
            vmem((2, NX, SLAB + 8, DK), F32), vmem((2, NX, SLAB + 8, DK), F32),
            vmem((2, SLAB + 8, DK), F32), vmem((2, NZ, SLAB + 8, DK), F32),
            vmem((NX, SLAB, DK), F32), vmem((NX, SLAB, DK), F32),
            vmem((2, NX, SLAB, DK), F32), vmem((2, NX, SLAB, DK), F32),
            vmem((NX, 6, T // 2, DK), F32), vmem((NX, ROWS, T), F32), vmem((NT, NX - 1, ROWS, T), F32),
            vmem((NZ, ROWS, DV), F32), vmem((NZ, ROWS, DV), F32),
            vmem((8, 128), F32), vmem((NT, 8, 128), F32),
            dma((6,)), dma((2, NX)), dma((2, NX)), dma((2, NZ)), dma((2, NZ)), dma((NX,)), dma((NX,)),
            dma((2, NX)), dma((2, NX)), dma((4, 6)), dma((4, 6)), dma((NX,)), dma((NX,)), dma((NX,)), dma((NX,)),
            dma((NX,)), dma((NX,)), dma((NZ,)), dma((NZ,)), dma((NT,)), dma((NT,)),
        ],
        compiler_params=pltpu.CompilerParams(collective_id=0, has_side_effects=True, vmem_limit_bytes=40 << 20),
        name="gla_backward",
    )(*args)
    outs = pl.pallas_call(
        finish,
        out_shape=tuple(jax.ShapeDtypeStruct(*s) for s in shapes),
        in_specs=[pl.BlockSpec(memory_space=pl.ANY)] * 5,
        out_specs=(hbm_spec,) * 5,
        scratch_shapes=[dma((5,))],
        compiler_params=pltpu.CompilerParams(vmem_limit_bytes=1 << 20),
        name="finish",
    )(*outs)
    return (*outs[:4], outs[4].reshape(ROWS))


def solution(mesh):
    in_specs = (P("sp", None), P("sp", "tp"), P("sp", "tp"), P(None, "tp"), P("sp", "tp"), P("sp", "tp"))
    out_specs = (P("sp", "tp"), P("sp", "tp"), P("sp", "tp"), P("sp", "tp"), P("sp"))
    return jax.shard_map(on_device, mesh=mesh, in_specs=in_specs, out_specs=out_specs, check_vma=False)
```

```python
import jax
import jax.numpy as jnp
from jax import lax
from jax.experimental import pallas as pl
from jax.experimental.pallas import tpu as pltpu
from jax.sharding import PartitionSpec as P

DK = 128
DV = 256
T = 256
BLK = 32
NB = T // BLK
NZ, NX, NT = 8, 4, 8
SLAB = DV // NX
ROWS = 64
MESH = pl.DeviceIdType.MESH
F32, BF16 = jnp.float32, jnp.bfloat16


def dot(a, b):
    return jnp.dot(a, b, preferred_element_type=F32)


def dot_nt(a, b):
    return lax.dot_general(a, b, (((1,), (1,)), ((), ())), preferred_element_type=F32)


def dot_tn(a, b):
    return lax.dot_general(a, b, (((0,), (0,)), ((), ())), preferred_element_type=F32)


def exact_sum(ones, a):
    hi = a.astype(BF16)
    rest = a - hi.astype(F32)
    mid = rest.astype(BF16)
    low = (rest - mid.astype(F32)).astype(BF16)
    return dot(ones, hi) + (dot(ones, mid) + dot(ones, low))


def kernel(
    x_hbm, q_hbm, k_hbm, w_hbm, g_hbm, do_hbm,
    dq_v, dk_v, dg_v, dwo_v, rn_v,
    x_v, q_v, k_v, w_v, g_v, do_v,
    xt_v, val_v, locs_v, adjs_v, as_v, vgs_v, xb_v,
    x1s, x1r, z2s, z2r, xis, xir, x3s, x3r, gx, xts, xg, dwp, rzr, tps, tpr,
    in_sem, x1_ss, x1_rs, z2_ss, z2_rs, xi_ss, xi_rs, x3_ss, x3_rs, gx_ss, gx_rs, xx_ss, xx_rs, xy_ss, xy_rs,
    xc_ss, xc_rs, rz_ss, rz_rs, tp_ss, tp_rs,
):
    sp, tp = lax.axis_index("sp"), lax.axis_index("tp")
    z, x = sp // NX, lax.rem(sp, NX)

    def x_dev(t):
        return {"sp": z * NX + t}

    def z_dev(t):
        return {"sp": t * NX + x}

    def tp_dev(t):
        return {"tp": t}

    barrier = pltpu.get_barrier_semaphore()
    for k in range(1, NX):
        pl.semaphore_signal(barrier, inc=1, device_id=x_dev(lax.rem(x + k, NX)), device_id_type=MESH)
    for k in range(1, NZ):
        pl.semaphore_signal(barrier, inc=1, device_id=z_dev(lax.rem(z + k, NZ)), device_id_type=MESH)
    for k in range(1, NT):
        pl.semaphore_signal(barrier, inc=1, device_id=tp_dev(lax.rem(tp + k, NT)), device_id_type=MESH)

    loads = [
        pltpu.make_async_copy(src, dst, in_sem.at[i])
        for i, (src, dst) in enumerate(
            ((g_hbm, g_v), (q_hbm, q_v), (do_hbm, do_v), (k_hbm, k_v), (x_hbm, x_v), (w_hbm, w_v))
        )
    ]
    for load in loads:
        load.start()

    started = []

    def go(cp):
        cp.start()
        started.append(cp)

    def remote(src, dst, ss, rs, dev):
        return pltpu.make_async_remote_copy(
            src_ref=src, dst_ref=dst, send_sem=ss, recv_sem=rs, device_id=dev, device_id_type=MESH
        )

    row = lax.broadcasted_iota(jnp.int32, (T, T), 0)
    col = lax.broadcasted_iota(jnp.int32, (T, T), 1)
    same = (row >> 5) == (col >> 5)
    lower = same & (col <= row)
    upper = same & (col >= row)

    loads[0].wait()
    c = exact_sum(lower.astype(BF16), g_v[...])
    c3 = c.reshape(NB, BLK, DK)
    ends = [c3[b, BLK - 1 : BLK, :] for b in range(NB)]
    before = [jnp.zeros((1, DK), F32)]
    for b in range(NB):
        before.append(before[-1] + ends[b])
    after = [jnp.zeros((1, DK), F32)]
    for b in reversed(range(1, NB)):
        after.append(after[-1] + ends[b])
    after = after[::-1]
    total = before[NB]

    def per_block(rows):
        return jnp.concatenate([jnp.broadcast_to(r, (BLK, DK)) for r in rows], axis=0)

    end_wide = per_block(ends)
    from_start = jnp.exp(c + per_block(before[:NB]))
    tail_log = end_wide - c
    to_end = jnp.exp(tail_log + per_block(after))
    span_decay = jnp.exp(total)

    loads[1].wait()
    loads[2].wait()
    qs = q_v[...].astype(F32) * (DK**-0.5)
    do = do_v[...]
    span_adj = dot_tn(do, (qs * from_start).astype(BF16))
    wide_decay = jnp.broadcast_to(span_decay, (8, DK))
    for s in range(NX):
        x1s[0, s, :SLAB, :] = span_adj[s * SLAB : (s + 1) * SLAB]
        x1s[0, s, SLAB:, :] = wide_decay

    loads[3].wait()
    kf = k_v[...].astype(F32)
    exp_c = jnp.exp(c)
    exp_nc = jnp.exp(-c)
    exp_tail = jnp.exp(tail_log)
    grown_q = (qs * exp_c).astype(BF16)
    shrunk_k = (kf * exp_nc).astype(BF16)
    tail_k = (kf * exp_tail).astype(BF16)
    k_end = kf * to_end
    adj = jnp.zeros((DV, DK), F32)
    for b in reversed(range(NB)):
        sl = slice(b * BLK, (b + 1) * BLK)
        adjs_v[b] = adj.astype(BF16)
        if b:
            adj = jnp.exp(ends[b]) * adj + dot_tn(do[sl], grown_q[sl])
    key_dots_t = jnp.where(upper, dot_nt(shrunk_k, grown_q), 0.0).astype(BF16)
    local_vg = dot(key_dots_t, do) + jnp.concatenate(
        [dot_nt(tail_k[b * BLK : (b + 1) * BLK], adjs_v[b]) for b in range(NB)], axis=0
    )
    gx[x, 4] = k_end[: T // 2]
    gx[x, 5] = k_end[T // 2 :]

    loads[4].wait()
    for zz in range(NZ):
        xt_v[:, zz] = x_v[:, zz * NX * ROWS : (zz + 1) * NX * ROWS].T.reshape(NX, ROWS, T)
    for t in range(NX):
        xts[t] = xt_v[t, tp].astype(F32)
    pl.semaphore_wait(barrier, NX - 1 + NZ - 1 + NT - 1)

    def x1_copy(i, k, src, slot, to):
        return remote(x1s.at[i, src], x1r.at[i, slot], x1_ss.at[i, k], x1_rs.at[i, k], x_dev(to))

    def x_leg(i):
        for k in (2, 1, 3):
            t = lax.rem(x + k, NX)
            go(x1_copy(i, k, t, x, t))
        x1r[i, x] = x1s[i, x]

    def x_leg_wait(i):
        for k in (2, 1, 3):
            t = lax.rem(x + NX - k, NX)
            x1_copy(i, k, t, t, t).wait_recv()

    x_leg(0)

    def xx_copy(k, t):
        return remote(xts.at[t], xg.at[tp, 3 - k], xx_ss.at[k], xx_rs.at[k], x_dev(t))

    for k in (1, 3, 2):
        go(xx_copy(k, lax.rem(x + k, NX)))

    right, left, far = lax.rem(x + 1, NX), lax.rem(x + 3, NX), lax.rem(x + 2, NX)
    ways = (right, left, right, left)

    def gx_copy(kind, piece, slot):
        ref = gx.at[slot, piece]
        return remote(ref, ref, gx_ss.at[kind, piece], gx_rs.at[kind, piece], x_dev(ways[kind]))

    def gx_own(first, second):
        for a, b in zip(first + second, second + first):
            go(gx_copy(0, a, x))
            go(gx_copy(1, b, x))

    def gx_forward(first, second):
        for a, b in zip(first, second):
            gx_copy(0, a, left).wait_recv()
            go(gx_copy(2, a, left))
            gx_copy(1, b, right).wait_recv()
            go(gx_copy(3, b, right))

    def gx_wait(first, second):
        for a, b in zip(first, second):
            gx_copy(0, b, left).wait_recv()
            gx_copy(1, a, right).wait_recv()
            gx_copy(2, a, far).wait_recv()
            gx_copy(3, b, far).wait_recv()

    loads[5].wait()
    val_v[...] = dot(x_v[...], w_v[...]).astype(BF16)
    v = val_v[...]
    span_state = dot_tn(v, k_end.astype(BF16))
    for s in range(NX):
        x1s[1, s, :SLAB, :] = span_state[s * SLAB : (s + 1) * SLAB]
        x1s[1, s, SLAB:, :] = wide_decay
    x_leg(1)

    def slab(i, t):
        return x1r[i, t, :SLAB, :]

    def slab_decay(i, t):
        return x1r[i, t, SLAB : SLAB + 1, :]

    def z_copy(i, k, t, slot):
        return remote(z2s.at[i], z2r.at[i, slot], z2_ss.at[i, k], z2_rs.at[i, k], z_dev(t))

    x_leg_wait(0)
    inner = [None] * NX
    inner[3] = jnp.zeros((SLAB, DK), F32)
    for t in (2, 1, 0):
        inner[t] = slab(0, t + 1) + slab_decay(0, t + 1) * inner[t + 1]
    row_decay = slab_decay(0, 0) * slab_decay(0, 1) * slab_decay(0, 2) * slab_decay(0, 3)
    z2s[0, :SLAB, :] = slab(0, 0) + slab_decay(0, 0) * inner[0]
    z2s[0, SLAB:, :] = jnp.broadcast_to(row_decay, (8, DK))
    for k in (4, 3, 5, 2, 6, 1, 7):
        @pl.when(z >= k)
        def _():
            z_copy(0, k, z - k, z).start()

    def xi_copy(k, src, slot, to):
        return remote(xis.at[src], xir.at[slot], xi_ss.at[k], xi_rs.at[k], x_dev(to))

    for t in range(NX):
        xis[t] = inner[t]
    for k in (2, 1, 3):
        t = lax.rem(x + k, NX)
        go(xi_copy(k, t, x, t))
    xir[x] = xis[x]
    gx_own((4,), (5,))

    sibling = tp + 1 - 2 * lax.rem(tp, 2)

    def xy_copy(j, k, slot, to):
        ref = xg.at[slot, k]
        return remote(ref, ref, xy_ss.at[j, k], xy_rs.at[j, k], tp_dev(to))

    def xc_copy(j, k, slot):
        ref = xg.at[slot, k]
        return remote(ref, ref, xc_ss.at[j, k], xc_rs.at[j, k], tp_dev(sibling))

    for k in (1, 3, 2):
        xx_copy(k, lax.rem(x + NX - k, NX)).wait_recv()
        for j in (2, 1, 3):
            go(xy_copy(j, 3 - k, tp, lax.rem(tp + 2 * j, NT)))
        go(xc_copy(0, 3 - k, tp))

    for k in (2, 1, 3):
        t = lax.rem(x + NX - k, NX)
        xi_copy(k, t, t, t).wait_recv()
    adj_row = xir[...].reshape(DV, DK)
    row_vg = local_vg + dot_nt(k_end.astype(BF16), adj_row.astype(BF16))
    for h in range(2):
        for p in range(2):
            gx[x, 2 * h + p] = row_vg[p * 128 : (p + 1) * 128, h * DK : (h + 1) * DK]
    gx_own((0,), (1,))
    gx_forward((4,), (5,))

    def adj_step(n, acc):
        t = NZ - 1 - n
        z_copy(0, t - z, t, t).wait_recv()
        return z2r[0, t, :SLAB, :] + z2r[0, t, SLAB : SLAB + 1, :] * acc

    x3s[0, 0] = lax.fori_loop(0, NZ - 1 - z, adj_step, jnp.zeros((SLAB, DK), F32))

    def x3_copy(i, k, src, slot, to):
        return remote(x3s.at[i, src], x3r.at[i, slot], x3_ss.at[i, k], x3_rs.at[i, k], x_dev(to))

    def x3_wait(i):
        for k in (2, 1, 3):
            t = lax.rem(x + NX - k, NX)
            x3_copy(i, k, 0, t, t).wait_recv()

    for k in (2, 1, 3):
        go(x3_copy(0, k, 0, x, lax.rem(x + k, NX)))
    x3r[0, x] = x3s[0, 0]

    gx_forward((0,), (1,))
    gx_own((2,), (3,))
    x_leg_wait(1)
    acc = slab(1, 0)
    for t in range(1, NX):
        acc = slab(1, t) + slab_decay(1, t) * acc
    z2s[1, :SLAB, :] = acc
    z2s[1, SLAB:, :] = jnp.broadcast_to(row_decay, (8, DK))
    for k in (4, 3, 5, 2, 6, 1, 7):
        @pl.when(z + k < NZ)
        def _():
            z_copy(1, k, z + k, z).start()

    for k in (1, 3, 2):
        for j in (1, 3, 2):
            slot = lax.rem(tp + NT - 2 * j, NT)
            xy_copy(j, 3 - k, slot, slot).wait_recv()
            go(xc_copy(j, 3 - k, slot))
    for j in (0, 1, 3, 2):
        for k in (1, 3, 2):
            xc_copy(j, 3 - k, lax.rem(sibling + NT - 2 * j, NT)).wait_recv()

    def columns(t):
        return pl.ds(pl.multiple_of(t * T, T), T)

    xb_v[:, :, columns(x)] = xt_v[x]
    for k in range(1, NX):
        xb_v[:, :, columns(lax.rem(x + k, NX))] = xg[:, k - 1].astype(BF16)

    def rz_copy(h, k, src, slot, to):
        return remote(dwp.at[h, src], rzr.at[h, slot], rz_ss.at[h, k], rz_rs.at[h, k], z_dev(to))

    late = []

    def half_product(h):
        for t in range(NX):
            k_t = gx[t, 4:6].reshape(T, DK).astype(BF16)
            a_t = as_v[t, h * DK : (h + 1) * DK].astype(BF16)
            vgs_v[t * T : (t + 1) * T] = (gx[t, 2 * h : 2 * h + 2].reshape(T, DK) + dot_nt(k_t, a_t)).astype(BF16)
        dwp[h] = dot(xb_v[...].reshape(NZ * ROWS, NX * T), vgs_v[...]).reshape(NZ, ROWS, DK)
        for k in (4, 3, 5, 2, 6, 1, 7):
            t = lax.rem(z + k, NZ)
            late.append(rz_copy(h, k, t, z, t))
            late[-1].start()

    gx_wait((4,), (5,))
    x3_wait(0)
    acc = x3r[0].reshape(DV, DK)
    for t in (3, 2, 1, 0):
        as_v[t] = acc
        if t:
            acc = slab_decay(0, t) * acc
    gx_wait((0,), (1,))
    half_product(0)
    gx_forward((2,), (3,))
    gx_wait((2,), (3,))
    half_product(1)
    adj_in = adj_row + as_v[x]
    adj_in16 = adj_in.astype(BF16)

    state = jnp.zeros((DV, DK), F32)
    for b in range(NB):
        sl = slice(b * BLK, (b + 1) * BLK)
        locs_v[b] = state.astype(BF16)
        if b < NB - 1:
            state = jnp.exp(ends[b]) * state + dot_tn(v[sl], tail_k[sl])
    out_dots = jnp.where(lower, dot_nt(do, v), 0.0).astype(BF16)
    out_dots_t = jnp.where(upper, dot_nt(v, do), 0.0).astype(BF16)
    local_qg = dot(out_dots, shrunk_k) + jnp.concatenate(
        [dot(do[b * BLK : (b + 1) * BLK], locs_v[b]) for b in range(NB)], axis=0
    )
    local_kg = exp_nc * dot(out_dots_t, grown_q) + exp_tail * jnp.concatenate(
        [dot(v[b * BLK : (b + 1) * BLK], adjs_v[b]) for b in range(NB)], axis=0
    )
    kg = local_kg + to_end * dot(v, adj_in16)
    dk_v[...] = kg.astype(BF16)

    def state_step(t, acc):
        z_copy(1, z - t, t, t).wait_recv()
        return z2r[1, t, :SLAB, :] + z2r[1, t, SLAB : SLAB + 1, :] * acc

    acc = lax.fori_loop(0, z, state_step, jnp.zeros((SLAB, DK), F32))
    for t in range(NX):
        x3s[1, t] = acc
        if t < NX - 1:
            acc = slab(1, t) + slab_decay(1, t) * acc
    for k in (2, 1, 3):
        t = lax.rem(x + k, NX)
        go(x3_copy(1, k, t, x, t))
    x3r[1, x] = x3s[1, x]
    x3_wait(1)
    state_in = x3r[1].reshape(DV, DK)
    qg = exp_c * local_qg + from_start * dot(do, state_in.astype(BF16))
    dq_v[...] = (qg * (DK**-0.5)).astype(BF16)
    carry = jnp.sum(adj_in * (span_state + span_decay * state_in), axis=0, keepdims=True)
    dg_v[...] = exact_sum((col >= row).astype(BF16), qs * qg - kf * kg) + carry
    for cp in started:
        cp.wait_send()
    for k in range(1, NZ):
        @pl.when(z >= k)
        def _():
            z_copy(0, k, z - k, z).wait_send()

        @pl.when(z + k < NZ)
        def _():
            z_copy(1, k, z + k, z).wait_send()

    squares = jnp.zeros((ROWS, DK), F32)
    for h in range(2):
        part = dwp[h, z]
        for k in (1, 7, 2, 6, 3, 5, 4):
            t = lax.rem(z + NZ - k, NZ)
            rz_copy(h, k, t, t, t).wait_recv()
            part = part + rzr[h, t]
        dwo_v[:, h * DK : (h + 1) * DK] = part
        squares = squares + part * part

    norms = jnp.sum(squares.T, axis=0, keepdims=True)
    tps[...] = jnp.broadcast_to(jnp.concatenate([norms, jnp.zeros((1, 64), F32)], axis=1), (8, 128))

    def tp_copy(k, slot, to):
        return remote(tps, tpr.at[slot], tp_ss.at[k], tp_rs.at[k], tp_dev(to))

    for k in range(1, NT):
        late.append(tp_copy(k, tp, lax.rem(tp + k, NT)))
        late[-1].start()
    acc = tps[0:1, :]
    for k in range(1, NT):
        t = lax.rem(tp + NT - k, NT)
        tp_copy(k, t, t).wait_recv()
        acc = acc + tpr[t, 0:1, :]
    rn_v[...] = acc[:, :ROWS]
    for cp in late:
        cp.wait_send()


def finish(*refs):
    ins, outs, sem = refs[:5], refs[5:10], refs[10]
    copies = [pltpu.make_async_copy(src, dst, sem.at[i]) for i, (src, dst) in enumerate(zip(ins, outs))]
    for cp in copies:
        cp.start()
    for cp in copies:
        cp.wait()


def on_device(block_input, queries, keys, w_value, log_decay, d_out):
    dma, vmem = pltpu.SemaphoreType.DMA, pltpu.VMEM
    hbm_spec, vmem_spec = pl.BlockSpec(memory_space=pltpu.HBM), pl.BlockSpec(memory_space=vmem)
    shapes = (((T, DK), BF16), ((T, DK), BF16), ((T, DK), F32), ((ROWS, DV), F32), ((1, ROWS), F32))
    args = [
        pltpu.with_memory_space_constraint(a, pltpu.HBM)
        for a in (block_input, queries, keys, w_value, log_decay, d_out)
    ]
    outs = pl.pallas_call(
        kernel,
        out_shape=tuple(vmem(*s) for s in shapes),
        in_specs=[hbm_spec] * 6,
        out_specs=(vmem_spec,) * 5,
        scratch_shapes=[
            vmem((T, 2048), BF16), vmem((T, DK), BF16), vmem((T, DK), BF16),
            vmem((2048, DV), BF16), vmem((T, DK), F32), vmem((T, DV), BF16),
            vmem((NX, NZ, ROWS, T), BF16), vmem((T, DV), BF16),
            vmem((NB, DV, DK), BF16), vmem((NB, DV, DK), BF16),
            vmem((NX, DV, DK), F32), vmem((NX * T, DK), BF16), vmem((NZ, ROWS, NX * T), BF16),
            vmem((2, NX, SLAB + 8, DK), F32), vmem((2, NX, SLAB + 8, DK), F32),
            vmem((2, SLAB + 8, DK), F32), vmem((2, NZ, SLAB + 8, DK), F32),
            vmem((NX, SLAB, DK), F32), vmem((NX, SLAB, DK), F32),
            vmem((2, NX, SLAB, DK), F32), vmem((2, NX, SLAB, DK), F32),
            vmem((NX, 6, T // 2, DK), F32), vmem((NX, ROWS, T), F32), vmem((NT, NX - 1, ROWS, T), F32),
            vmem((2, NZ, ROWS, DK), F32), vmem((2, NZ, ROWS, DK), F32),
            vmem((8, 128), F32), vmem((NT, 8, 128), F32),
            dma((6,)), dma((2, NX)), dma((2, NX)), dma((2, NZ)), dma((2, NZ)), dma((NX,)), dma((NX,)),
            dma((2, NX)), dma((2, NX)), dma((4, 6)), dma((4, 6)), dma((NX,)), dma((NX,)), dma((NX, 3)), dma((NX, 3)),
            dma((NX, 3)), dma((NX, 3)), dma((2, NZ)), dma((2, NZ)), dma((NT,)), dma((NT,)),
        ],
        compiler_params=pltpu.CompilerParams(collective_id=0, has_side_effects=True, vmem_limit_bytes=40 << 20),
        name="gla_backward",
    )(*args)
    outs = pl.pallas_call(
        finish,
        out_shape=tuple(jax.ShapeDtypeStruct(*s) for s in shapes),
        in_specs=[pl.BlockSpec(memory_space=pl.ANY)] * 5,
        out_specs=(hbm_spec,) * 5,
        scratch_shapes=[dma((5,))],
        compiler_params=pltpu.CompilerParams(vmem_limit_bytes=1 << 20),
        name="finish",
    )(*outs)
    return (*outs[:4], outs[4].reshape(ROWS))


def solution(mesh):
    in_specs = (P("sp", None), P("sp", "tp"), P("sp", "tp"), P(None, "tp"), P("sp", "tp"), P("sp", "tp"))
    out_specs = (P("sp", "tp"), P("sp", "tp"), P("sp", "tp"), P("sp", "tp"), P("sp"))
    return jax.shard_map(on_device, mesh=mesh, in_specs=in_specs, out_specs=out_specs, check_vma=False)
```

```python
import jax
import jax.numpy as jnp
from jax import lax
from jax.experimental import pallas as pl
from jax.experimental.pallas import tpu as pltpu
from jax.sharding import PartitionSpec as P

DK = 128
DV = 256
T = 256
BLK = 32
NB = T // BLK
NZ, NX, NT = 8, 4, 8
SLAB = DV // NX
ROWS = 64
X1, Z2, XI, X3, GX, XX, XY, XC, RZ, TP = 0, 2, 3, 4, 6, 7, 8, 9, 10, 12
MESH = pl.DeviceIdType.MESH
F32, BF16 = jnp.float32, jnp.bfloat16


def dot(a, b):
    return jnp.dot(a, b, preferred_element_type=F32)


def dot_nt(a, b):
    return lax.dot_general(a, b, (((1,), (1,)), ((), ())), preferred_element_type=F32)


def dot_tn(a, b):
    return lax.dot_general(a, b, (((0,), (0,)), ((), ())), preferred_element_type=F32)


def exact_sum(ones, a):
    hi = a.astype(BF16)
    rest = a - hi.astype(F32)
    mid = rest.astype(BF16)
    low = (rest - mid.astype(F32)).astype(BF16)
    return dot(ones, hi) + (dot(ones, mid) + dot(ones, low))


def kernel(
    x_hbm, q_hbm, k_hbm, w_hbm, g_hbm, do_hbm,
    dq_o, dk_o, dg_o, dwo_o, rn_o,
    x_v, q_v, k_v, w_v, g_v, do_v, dq_v, dk_v, dg_v, dwo_v, rn_v,
    xt_v, val_v, locs_v, adjs_v, as_v, vgs_v, xb_v,
    x1s, x1r, z2s, z2r, xis, xir, x3s, x3r, gx, xts, xg, dwp, rzr, tps, tpr,
    in_sem, out_sem, sent, x1_rs, z2_rs, xi_rs, x3_rs, gx_rs, gx_rest, xx_rs, xy_rs, xc_rs, rz_rs, tp_rs,
):
    sp, tp = lax.axis_index("sp"), lax.axis_index("tp")
    z, x = sp // NX, lax.rem(sp, NX)

    def x_dev(t):
        return {"sp": z * NX + t}

    def z_dev(t):
        return {"sp": t * NX + x}

    def tp_dev(t):
        return {"tp": t}

    barrier = pltpu.get_barrier_semaphore()
    for k in range(1, NX):
        pl.semaphore_signal(barrier, inc=1, device_id=x_dev(lax.rem(x + k, NX)), device_id_type=MESH)
    for k in range(1, NZ):
        pl.semaphore_signal(barrier, inc=1, device_id=z_dev(lax.rem(z + k, NZ)), device_id_type=MESH)
    for k in range(1, NT):
        pl.semaphore_signal(barrier, inc=1, device_id=tp_dev(lax.rem(tp + k, NT)), device_id_type=MESH)

    loads = [
        pltpu.make_async_copy(src, dst, in_sem.at[i])
        for i, (src, dst) in enumerate(
            ((g_hbm, g_v), (q_hbm, q_v), (do_hbm, do_v), (k_hbm, k_v), (x_hbm, x_v), (w_hbm, w_v))
        )
    ]
    for load in loads:
        load.start()

    def remote(src, dst, ss, rs, dev):
        return pltpu.make_async_remote_copy(
            src_ref=src, dst_ref=dst, send_sem=ss, recv_sem=rs, device_id=dev, device_id_type=MESH
        )

    row = lax.broadcasted_iota(jnp.int32, (T, T), 0)
    col = lax.broadcasted_iota(jnp.int32, (T, T), 1)
    same = (row >> 5) == (col >> 5)
    lower = same & (col <= row)
    upper = same & (col >= row)

    loads[0].wait()
    c = exact_sum(lower.astype(BF16), g_v[...])
    c3 = c.reshape(NB, BLK, DK)
    ends = [c3[b, BLK - 1 : BLK, :] for b in range(NB)]
    before = [jnp.zeros((1, DK), F32)]
    for b in range(NB):
        before.append(before[-1] + ends[b])
    after = [jnp.zeros((1, DK), F32)]
    for b in reversed(range(1, NB)):
        after.append(after[-1] + ends[b])
    after = after[::-1]
    total = before[NB]

    def per_block(rows):
        return jnp.concatenate([jnp.broadcast_to(r, (BLK, DK)) for r in rows], axis=0)

    end_wide = per_block(ends)
    from_start = jnp.exp(c + per_block(before[:NB]))
    tail_log = end_wide - c
    to_end = jnp.exp(tail_log + per_block(after))
    span_decay = jnp.exp(total)

    loads[1].wait()
    loads[2].wait()
    qs = q_v[...].astype(F32) * (DK**-0.5)
    do = do_v[...]
    span_adj = dot_tn(do, (qs * from_start).astype(BF16))
    wide_decay = jnp.broadcast_to(span_decay, (8, DK))
    for s in range(NX):
        x1s[0, s, :SLAB, :] = span_adj[s * SLAB : (s + 1) * SLAB]
        x1s[0, s, SLAB:, :] = wide_decay

    loads[3].wait()
    kf = k_v[...].astype(F32)
    exp_c = jnp.exp(c)
    exp_nc = jnp.exp(-c)
    exp_tail = jnp.exp(tail_log)
    grown_q = (qs * exp_c).astype(BF16)
    shrunk_k = (kf * exp_nc).astype(BF16)
    tail_k = (kf * exp_tail).astype(BF16)
    k_end = kf * to_end
    adj = jnp.zeros((DV, DK), F32)
    for b in reversed(range(NB)):
        sl = slice(b * BLK, (b + 1) * BLK)
        adjs_v[b] = adj.astype(BF16)
        if b:
            adj = jnp.exp(ends[b]) * adj + dot_tn(do[sl], grown_q[sl])
    key_dots_t = jnp.where(upper, dot_nt(shrunk_k, grown_q), 0.0).astype(BF16)
    local_vg = dot(key_dots_t, do) + jnp.concatenate(
        [dot_nt(tail_k[b * BLK : (b + 1) * BLK], adjs_v[b]) for b in range(NB)], axis=0
    )
    gx[x, 4] = k_end[: T // 2]
    gx[x, 5] = k_end[T // 2 :]

    loads[4].wait()
    for zz in range(NZ):
        xt_v[:, zz] = x_v[:, zz * NX * ROWS : (zz + 1) * NX * ROWS].T.reshape(NX, ROWS, T)
    for t in range(NX):
        xts[t] = xt_v[t, tp].astype(F32)
    pl.semaphore_wait(barrier, NX - 1 + NZ - 1 + NT - 1)

    def x1_copy(i, src, slot, to):
        return remote(x1s.at[i, src], x1r.at[i, slot], sent.at[X1 + i], x1_rs.at[i], x_dev(to))

    def x_leg(i):
        for k in (2, 1, 3):
            t = lax.rem(x + k, NX)
            x1_copy(i, t, x, t).start()
        x1r[i, x] = x1s[i, x]

    def arrived(ref, sem):
        remote(ref, ref, sent.at[0], sem, x_dev(x)).wait_recv()

    def left_here(ref, sem):
        remote(ref, ref, sem, x1_rs.at[0], x_dev(x)).wait_send()

    def x_leg_wait(i):
        arrived(x1r.at[i, pl.ds(0, 3)], x1_rs.at[i])

    x_leg(0)

    def xx_copy(k, t):
        return remote(xts.at[t], xg.at[tp, 3 - k], sent.at[XX], xx_rs.at[k - 1], x_dev(t))

    for k in (1, 3, 2):
        xx_copy(k, lax.rem(x + k, NX)).start()

    right, left, far = lax.rem(x + 1, NX), lax.rem(x + 3, NX), lax.rem(x + 2, NX)
    ways = (right, left, right, left)

    def gx_copy(kind, piece, slot, sem):
        ref = gx.at[slot, piece]
        return remote(ref, ref, sent.at[GX], sem, x_dev(ways[kind]))

    stages = ((4, 5), (0, 1), (2, 3))

    def gx_own(stage):
        a, b = stages[stage]
        gx_copy(0, a, x, gx_rs.at[0, stage]).start()
        gx_copy(1, b, x, gx_rs.at[1, stage]).start()
        gx_copy(0, b, x, gx_rest.at[stage]).start()
        gx_copy(1, a, x, gx_rest.at[stage]).start()

    def gx_forward(stage):
        a, b = stages[stage]
        gx_copy(0, a, left, gx_rs.at[0, stage]).wait_recv()
        gx_copy(2, a, left, gx_rest.at[stage]).start()
        gx_copy(1, b, right, gx_rs.at[1, stage]).wait_recv()
        gx_copy(3, b, right, gx_rest.at[stage]).start()

    def gx_wait(stage):
        arrived(gx.at[0, pl.ds(0, 4)], gx_rest.at[stage])

    loads[5].wait()
    val_v[...] = dot(x_v[...], w_v[...]).astype(BF16)
    v = val_v[...]
    span_state = dot_tn(v, k_end.astype(BF16))
    for s in range(NX):
        x1s[1, s, :SLAB, :] = span_state[s * SLAB : (s + 1) * SLAB]
        x1s[1, s, SLAB:, :] = wide_decay
    x_leg(1)

    def slab(i, t):
        return x1r[i, t, :SLAB, :]

    def slab_decay(i, t):
        return x1r[i, t, SLAB : SLAB + 1, :]

    def z_copy(i, t, slot):
        return remote(z2s.at[i], z2r.at[i, slot], sent.at[Z2], z2_rs.at[slot], z_dev(t))

    x_leg_wait(0)
    inner = [None] * NX
    inner[3] = jnp.zeros((SLAB, DK), F32)
    for t in (2, 1, 0):
        inner[t] = slab(0, t + 1) + slab_decay(0, t + 1) * inner[t + 1]
    row_decay = slab_decay(0, 0) * slab_decay(0, 1) * slab_decay(0, 2) * slab_decay(0, 3)
    z2s[0, :SLAB, :] = slab(0, 0) + slab_decay(0, 0) * inner[0]
    z2s[0, SLAB:, :] = jnp.broadcast_to(row_decay, (8, DK))
    for k in (4, 3, 5, 2, 6, 1, 7):
        @pl.when(z >= k)
        def _():
            z_copy(0, z - k, z).start()

    def xi_copy(src, slot, to):
        return remote(xis.at[src], xir.at[slot], sent.at[XI], xi_rs.at[0], x_dev(to))

    for t in range(NX):
        xis[t] = inner[t]
    for k in (2, 1, 3):
        t = lax.rem(x + k, NX)
        xi_copy(t, x, t).start()
    xir[x] = xis[x]
    gx_own(0)

    sibling = tp + 1 - 2 * lax.rem(tp, 2)

    def xy_copy(j, k, slot, to):
        ref = xg.at[slot, k]
        return remote(ref, ref, sent.at[XY], xy_rs.at[j - 1, k], tp_dev(to))

    def xc_copy(k, slot):
        ref = xg.at[slot, k]
        return remote(ref, ref, sent.at[XC], xc_rs.at[0], tp_dev(sibling))

    for k in (1, 3, 2):
        xx_copy(k, lax.rem(x + NX - k, NX)).wait_recv()
        for j in (2, 1, 3):
            xy_copy(j, 3 - k, tp, lax.rem(tp + 2 * j, NT)).start()
        xc_copy(3 - k, tp).start()

    arrived(xir.at[pl.ds(0, 3)], xi_rs.at[0])
    adj_row = xir[...].reshape(DV, DK)
    row_vg = local_vg + dot_nt(k_end.astype(BF16), adj_row.astype(BF16))
    for h in range(2):
        for p in range(2):
            gx[x, 2 * h + p] = row_vg[p * 128 : (p + 1) * 128, h * DK : (h + 1) * DK]
    gx_own(1)
    gx_forward(0)

    def adj_step(n, acc):
        t = NZ - 1 - n
        z_copy(0, t, t).wait_recv()
        return z2r[0, t, :SLAB, :] + z2r[0, t, SLAB : SLAB + 1, :] * acc

    x3s[0, 0] = lax.fori_loop(0, NZ - 1 - z, adj_step, jnp.zeros((SLAB, DK), F32))

    def x3_copy(i, src, slot, to):
        return remote(x3s.at[i, src], x3r.at[i, slot], sent.at[X3 + i], x3_rs.at[i], x_dev(to))

    def x3_wait(i):
        arrived(x3r.at[i, pl.ds(0, 3)], x3_rs.at[i])

    for k in (2, 1, 3):
        x3_copy(0, 0, x, lax.rem(x + k, NX)).start()
    x3r[0, x] = x3s[0, 0]

    gx_forward(1)
    gx_own(2)
    x_leg_wait(1)
    acc = slab(1, 0)
    for t in range(1, NX):
        acc = slab(1, t) + slab_decay(1, t) * acc
    z2s[1, :SLAB, :] = acc
    z2s[1, SLAB:, :] = jnp.broadcast_to(row_decay, (8, DK))
    for k in (4, 3, 5, 2, 6, 1, 7):
        @pl.when(z + k < NZ)
        def _():
            z_copy(1, z + k, z).start()

    for k in (1, 3, 2):
        for j in (1, 3, 2):
            slot = lax.rem(tp + NT - 2 * j, NT)
            xy_copy(j, 3 - k, slot, slot).wait_recv()
            xc_copy(3 - k, slot).start()
    arrived(xg.at[pl.ds(0, 4)], xc_rs.at[0])

    def columns(t):
        return pl.ds(pl.multiple_of(t * T, T), T)

    xb_v[:, :, columns(x)] = xt_v[x]
    for k in range(1, NX):
        xb_v[:, :, columns(lax.rem(x + k, NX))] = xg[:, k - 1].astype(BF16)

    def rz_copy(h, src, slot, to):
        return remote(dwp.at[h, src], rzr.at[h, slot], sent.at[RZ + h], rz_rs.at[h], z_dev(to))

    def half_product(h):
        for t in range(NX):
            k_t = gx[t, 4:6].reshape(T, DK).astype(BF16)
            a_t = as_v[t, h * DK : (h + 1) * DK].astype(BF16)
            vgs_v[t * T : (t + 1) * T] = (gx[t, 2 * h : 2 * h + 2].reshape(T, DK) + dot_nt(k_t, a_t)).astype(BF16)
        dwp[h] = dot(xb_v[...].reshape(NZ * ROWS, NX * T), vgs_v[...]).reshape(NZ, ROWS, DK)
        for k in (4, 3, 5, 2, 6, 1, 7):
            t = lax.rem(z + k, NZ)
            rz_copy(h, t, z, t).start()

    gx_wait(0)
    x3_wait(0)
    acc = x3r[0].reshape(DV, DK)
    for t in (3, 2, 1, 0):
        as_v[t] = acc
        if t:
            acc = slab_decay(0, t) * acc
    gx_wait(1)
    half_product(0)
    gx_forward(2)
    gx_wait(2)
    half_product(1)
    adj_in = adj_row + as_v[x]
    adj_in16 = adj_in.astype(BF16)

    state = jnp.zeros((DV, DK), F32)
    for b in range(NB):
        sl = slice(b * BLK, (b + 1) * BLK)
        locs_v[b] = state.astype(BF16)
        if b < NB - 1:
            state = jnp.exp(ends[b]) * state + dot_tn(v[sl], tail_k[sl])
    out_dots = jnp.where(lower, dot_nt(do, v), 0.0).astype(BF16)
    out_dots_t = jnp.where(upper, dot_nt(v, do), 0.0).astype(BF16)
    local_qg = dot(out_dots, shrunk_k) + jnp.concatenate(
        [dot(do[b * BLK : (b + 1) * BLK], locs_v[b]) for b in range(NB)], axis=0
    )
    local_kg = exp_nc * dot(out_dots_t, grown_q) + exp_tail * jnp.concatenate(
        [dot(v[b * BLK : (b + 1) * BLK], adjs_v[b]) for b in range(NB)], axis=0
    )
    kg = local_kg + to_end * dot(v, adj_in16)
    dk_v[...] = kg.astype(BF16)

    def state_step(t, acc):
        z_copy(1, t, t).wait_recv()
        return z2r[1, t, :SLAB, :] + z2r[1, t, SLAB : SLAB + 1, :] * acc

    acc = lax.fori_loop(0, z, state_step, jnp.zeros((SLAB, DK), F32))
    for t in range(NX):
        x3s[1, t] = acc
        if t < NX - 1:
            acc = slab(1, t) + slab_decay(1, t) * acc
    for k in (2, 1, 3):
        t = lax.rem(x + k, NX)
        x3_copy(1, t, x, t).start()
    x3r[1, x] = x3s[1, x]
    x3_wait(1)
    state_in = x3r[1].reshape(DV, DK)
    qg = exp_c * local_qg + from_start * dot(do, state_in.astype(BF16))
    dq_v[...] = (qg * (DK**-0.5)).astype(BF16)
    carry = jnp.sum(adj_in * (span_state + span_decay * state_in), axis=0, keepdims=True)
    dg_v[...] = exact_sum((col >= row).astype(BF16), qs * qg - kf * kg) + carry
    stores = [
        pltpu.make_async_copy(src, dst, out_sem.at[i])
        for i, (src, dst) in enumerate(((dq_v, dq_o), (dk_v, dk_o), (dg_v, dg_o), (dwo_v, dwo_o), (rn_v, rn_o)))
    ]
    for store in stores[:3]:
        store.start()

    left_here(x1s.at[0, pl.ds(0, 3)], sent.at[X1])
    left_here(x1s.at[1, pl.ds(0, 3)], sent.at[X1 + 1])
    left_here(z2r.at[0, pl.ds(0, 7)], sent.at[Z2])
    left_here(xis.at[pl.ds(0, 3)], sent.at[XI])
    left_here(x3r.at[0, pl.ds(0, 3)], sent.at[X3])
    left_here(x3r.at[1, pl.ds(0, 3)], sent.at[X3 + 1])
    left_here(gx.at[pl.ds(0, 3)], sent.at[GX])
    left_here(xts.at[pl.ds(0, 3)], sent.at[XX])
    left_here(xg.at[pl.ds(0, 3)], sent.at[XY])
    left_here(xg.at[pl.ds(0, 4)], sent.at[XC])
    for store in stores[:3]:
        store.wait()

    squares = jnp.zeros((ROWS, DK), F32)
    for h in range(2):
        part = dwp[h, z]
        arrived(rzr.at[h, pl.ds(0, 7)], rz_rs.at[h])
        for k in range(1, NZ):
            part = part + rzr[h, lax.rem(z + k, NZ)]
        dwo_v[:, h * DK : (h + 1) * DK] = part
        squares = squares + part * part
    stores[3].start()

    norms = jnp.sum(squares.T, axis=0, keepdims=True)
    tps[...] = jnp.broadcast_to(jnp.concatenate([norms, jnp.zeros((1, 64), F32)], axis=1), (8, 128))

    def tp_copy(slot, to):
        return remote(tps, tpr.at[slot], sent.at[TP], tp_rs.at[0], tp_dev(to))

    for k in range(1, NT):
        tp_copy(tp, lax.rem(tp + k, NT)).start()
    left_here(dwp.at[0, pl.ds(0, 7)], sent.at[RZ])
    left_here(dwp.at[1, pl.ds(0, 7)], sent.at[RZ + 1])
    stores[3].wait()
    left_here(tpr.at[pl.ds(0, 7)], sent.at[TP])
    arrived(tpr.at[pl.ds(0, 7)], tp_rs.at[0])
    acc = tps[0:1, :]
    for k in range(1, NT):
        t = lax.rem(tp + NT - k, NT)
        acc = acc + tpr[t, 0:1, :]
    rn_v[...] = acc[:, :ROWS]
    stores[4].start()
    stores[4].wait()


def finish(*refs):
    ins, outs, sem = refs[:5], refs[5:10], refs[10]
    copies = [pltpu.make_async_copy(src, dst, sem.at[i]) for i, (src, dst) in enumerate(zip(ins, outs))]
    for cp in copies:
        cp.start()
    for cp in copies:
        cp.wait()


def on_device(block_input, queries, keys, w_value, log_decay, d_out):
    dma, vmem = pltpu.SemaphoreType.DMA, pltpu.VMEM
    hbm_spec = pl.BlockSpec(memory_space=pltpu.HBM)
    shapes = (((T, DK), BF16), ((T, DK), BF16), ((T, DK), F32), ((ROWS, DV), F32), ((1, ROWS), F32))
    args = [
        pltpu.with_memory_space_constraint(a, pltpu.HBM)
        for a in (block_input, queries, keys, w_value, log_decay, d_out)
    ]
    outs = pl.pallas_call(
        kernel,
        out_shape=tuple(vmem(*s) for s in shapes),
        in_specs=[hbm_spec] * 6,
        out_specs=(pl.BlockSpec(memory_space=pl.ANY),) * 5,
        scratch_shapes=[
            vmem((T, 2048), BF16), vmem((T, DK), BF16), vmem((T, DK), BF16),
            vmem((2048, DV), BF16), vmem((T, DK), F32), vmem((T, DV), BF16),
            vmem((T, DK), BF16), vmem((T, DK), BF16), vmem((T, DK), F32),
            vmem((ROWS, DV), F32), vmem((1, ROWS), F32),
            vmem((NX, NZ, ROWS, T), BF16), vmem((T, DV), BF16),
            vmem((NB, DV, DK), BF16), vmem((NB, DV, DK), BF16),
            vmem((NX, DV, DK), F32), vmem((NX * T, DK), BF16), vmem((NZ, ROWS, NX * T), BF16),
            vmem((2, NX, SLAB + 8, DK), F32), vmem((2, NX, SLAB + 8, DK), F32),
            vmem((2, SLAB + 8, DK), F32), vmem((2, NZ, SLAB + 8, DK), F32),
            vmem((NX, SLAB, DK), F32), vmem((NX, SLAB, DK), F32),
            vmem((2, NX, SLAB, DK), F32), vmem((2, NX, SLAB, DK), F32),
            vmem((NX, 6, T // 2, DK), F32), vmem((NX, ROWS, T), F32), vmem((NT, NX - 1, ROWS, T), F32),
            vmem((2, NZ, ROWS, DK), F32), vmem((2, NZ, ROWS, DK), F32),
            vmem((8, 128), F32), vmem((NT, 8, 128), F32),
            dma((6,)), dma((5,)), dma((13,)), dma((2,)), dma((NZ,)), dma((1,)), dma((2,)), dma((2, 3)), dma((3,)),
            dma((3,)), dma((3, 3)), dma((1,)), dma((2,)), dma((1,)),
        ],
        compiler_params=pltpu.CompilerParams(collective_id=0, has_side_effects=True, vmem_limit_bytes=40 << 20),
        name="gla_backward",
    )(*args)
    outs = pl.pallas_call(
        finish,
        out_shape=tuple(jax.ShapeDtypeStruct(*s) for s in shapes),
        in_specs=[pl.BlockSpec(memory_space=pl.ANY)] * 5,
        out_specs=(hbm_spec,) * 5,
        scratch_shapes=[dma((5,))],
        compiler_params=pltpu.CompilerParams(vmem_limit_bytes=1 << 20),
        name="finish",
    )(*outs)
    return (*outs[:4], outs[4].reshape(ROWS))


def solution(mesh):
    in_specs = (P("sp", None), P("sp", "tp"), P("sp", "tp"), P(None, "tp"), P("sp", "tp"), P("sp", "tp"))
    out_specs = (P("sp", "tp"), P("sp", "tp"), P("sp", "tp"), P("sp", "tp"), P("sp"))
    return jax.shard_map(on_device, mesh=mesh, in_specs=in_specs, out_specs=out_specs, check_vma=False)
```

```python
import jax
import jax.numpy as jnp
from jax import lax
from jax.experimental import pallas as pl
from jax.experimental.pallas import tpu as pltpu
from jax.sharding import PartitionSpec as P

DK = 128
DV = 256
T = 256
BLK = 32
NB = T // BLK
NZ, NX, NT = 8, 4, 8
SLAB = DV // NX
ROWS = 64
X1, Z2, XI, X3, GX, XX, XY, XC, RZ, TP = 0, 2, 3, 4, 6, 7, 8, 9, 10, 12
MESH = pl.DeviceIdType.MESH
F32, BF16 = jnp.float32, jnp.bfloat16


def dot(a, b):
    return jnp.dot(a, b, preferred_element_type=F32)


def dot_nt(a, b):
    return lax.dot_general(a, b, (((1,), (1,)), ((), ())), preferred_element_type=F32)


def dot_tn(a, b):
    return lax.dot_general(a, b, (((0,), (0,)), ((), ())), preferred_element_type=F32)


def exact_sum(ones, a):
    hi = a.astype(BF16)
    rest = a - hi.astype(F32)
    mid = rest.astype(BF16)
    low = (rest - mid.astype(F32)).astype(BF16)
    return dot(ones, hi) + (dot(ones, mid) + dot(ones, low))


def kernel(
    x_hbm, q_hbm, k_hbm, w_hbm, g_hbm, do_hbm,
    dq_o, dk_o, dg_o, dwo_o, rn_o,
    x_v, q_v, k_v, w_v, g_v, do_v, dq_v, dk_v, dg_v, dwo_v, rn_v,
    xt_v, val_v, locs_v, adjs_v, as_v, xb_v,
    x1s, x1r, z2s, z2r, xis, xir, x3s, x3r, gx, xts, xg, dwp, rzr, tps, tpr,
    in_sem, out_sem, sent, x1_rs, z2_rs, xi_rs, x3_rs, gx_rs, gx_rest, gx_far, xx_rs, xy_rs, xc_rs, rz_rs, tp_rs,
):
    sp, tp = lax.axis_index("sp"), lax.axis_index("tp")
    z, x = sp // NX, lax.rem(sp, NX)

    def x_dev(t):
        return {"sp": z * NX + t}

    def z_dev(t):
        return {"sp": t * NX + x}

    def tp_dev(t):
        return {"tp": t}

    barrier = pltpu.get_barrier_semaphore()
    for k in range(1, NX):
        pl.semaphore_signal(barrier, inc=1, device_id=x_dev(lax.rem(x + k, NX)), device_id_type=MESH)
    for k in range(1, NZ):
        pl.semaphore_signal(barrier, inc=1, device_id=z_dev(lax.rem(z + k, NZ)), device_id_type=MESH)
    for k in range(1, NT):
        pl.semaphore_signal(barrier, inc=1, device_id=tp_dev(lax.rem(tp + k, NT)), device_id_type=MESH)

    loads = [
        pltpu.make_async_copy(src, dst, in_sem.at[i])
        for i, (src, dst) in enumerate(
            ((g_hbm, g_v), (q_hbm, q_v), (do_hbm, do_v), (k_hbm, k_v), (x_hbm, x_v), (w_hbm, w_v))
        )
    ]
    for load in loads:
        load.start()

    def remote(src, dst, ss, rs, dev):
        return pltpu.make_async_remote_copy(
            src_ref=src, dst_ref=dst, send_sem=ss, recv_sem=rs, device_id=dev, device_id_type=MESH
        )

    row = lax.broadcasted_iota(jnp.int32, (T, T), 0)
    col = lax.broadcasted_iota(jnp.int32, (T, T), 1)
    same = (row >> 5) == (col >> 5)
    lower = same & (col <= row)
    upper = same & (col >= row)

    loads[0].wait()
    c = exact_sum(lower.astype(BF16), g_v[...])
    c3 = c.reshape(NB, BLK, DK)
    ends = [c3[b, BLK - 1 : BLK, :] for b in range(NB)]
    before = [jnp.zeros((1, DK), F32)]
    for b in range(NB):
        before.append(before[-1] + ends[b])
    after = [jnp.zeros((1, DK), F32)]
    for b in reversed(range(1, NB)):
        after.append(after[-1] + ends[b])
    after = after[::-1]
    total = before[NB]

    def per_block(rows):
        return jnp.concatenate([jnp.broadcast_to(r, (BLK, DK)) for r in rows], axis=0)

    end_wide = per_block(ends)
    from_start = jnp.exp(c + per_block(before[:NB]))
    tail_log = end_wide - c
    to_end = jnp.exp(tail_log + per_block(after))
    span_decay = jnp.exp(total)

    loads[1].wait()
    loads[2].wait()
    qs = q_v[...].astype(F32) * (DK**-0.5)
    do = do_v[...]
    span_adj = dot_tn(do, (qs * from_start).astype(BF16))
    wide_decay = jnp.broadcast_to(span_decay, (8, DK))
    for s in range(NX):
        x1s[0, s, :SLAB, :] = span_adj[s * SLAB : (s + 1) * SLAB]
        x1s[0, s, SLAB:, :] = wide_decay

    pl.semaphore_wait(barrier, NX - 1 + NZ - 1 + NT - 1)

    def x1_copy(i, src, slot, to):
        return remote(x1s.at[i, src], x1r.at[i, slot], sent.at[X1 + i], x1_rs.at[i], x_dev(to))

    def x_leg(i):
        for k in (2, 1, 3):
            t = lax.rem(x + k, NX)
            x1_copy(i, t, x, t).start()
        x1r[i, x] = x1s[i, x]

    def arrived(ref, sem):
        remote(ref, ref, sent.at[0], sem, x_dev(x)).wait_recv()

    def left_here(ref, sem):
        remote(ref, ref, sem, x1_rs.at[0], x_dev(x)).wait_send()

    def x_leg_wait(i):
        arrived(x1r.at[i, pl.ds(0, 3)], x1_rs.at[i])

    x_leg(0)

    loads[4].wait()
    for zz in range(NZ):
        xt_v[:, zz] = x_v[:, zz * NX * ROWS : (zz + 1) * NX * ROWS].T.reshape(NX, ROWS, T)
    for t in range(NX):
        xts[t] = xt_v[t, tp].astype(F32)

    def xx_copy(k, t):
        return remote(xts.at[t], xg.at[tp, 3 - k], sent.at[XX], xx_rs.at[k - 1], x_dev(t))

    for k in (1, 3, 2):
        xx_copy(k, lax.rem(x + k, NX)).start()

    right, left, far = lax.rem(x + 1, NX), lax.rem(x + 3, NX), lax.rem(x + 2, NX)
    ways = (right, left, right, left)

    def gx_copy(kind, piece, slot, sem):
        ref = gx.at[slot, piece]
        return remote(ref, ref, sent.at[GX], sem, x_dev(ways[kind]))

    stages = ((4, 5), (0, 1), (2, 3))

    def gx_own(stage):
        a, b = stages[stage]
        gx_copy(0, a, x, gx_rs.at[0, stage]).start()
        gx_copy(1, b, x, gx_rs.at[1, stage]).start()
        gx_copy(0, b, x, gx_rest.at[stage]).start()
        gx_copy(1, a, x, gx_rest.at[stage]).start()

    def gx_forward(stage):
        a, b = stages[stage]
        gx_copy(0, a, left, gx_rs.at[0, stage]).wait_recv()
        gx_copy(2, a, left, gx_far.at[stage]).start()
        gx_copy(1, b, right, gx_rs.at[1, stage]).wait_recv()
        gx_copy(3, b, right, gx_far.at[stage]).start()

    def gx_wait(sems, stage):
        arrived(gx.at[0, pl.ds(0, 2)], sems.at[stage])

    loads[3].wait()
    kf = k_v[...].astype(F32)
    exp_c = jnp.exp(c)
    exp_nc = jnp.exp(-c)
    exp_tail = jnp.exp(tail_log)
    grown_q = (qs * exp_c).astype(BF16)
    shrunk_k = (kf * exp_nc).astype(BF16)
    tail_k = (kf * exp_tail).astype(BF16)
    k_end = kf * to_end
    adj = jnp.zeros((DV, DK), F32)
    for b in reversed(range(NB)):
        sl = slice(b * BLK, (b + 1) * BLK)
        adjs_v[b] = adj.astype(BF16)
        if b:
            adj = jnp.exp(ends[b]) * adj + dot_tn(do[sl], grown_q[sl])
    key_dots_t = jnp.where(upper, dot_nt(shrunk_k, grown_q), 0.0).astype(BF16)
    local_vg = dot(key_dots_t, do) + jnp.concatenate(
        [dot_nt(tail_k[b * BLK : (b + 1) * BLK], adjs_v[b]) for b in range(NB)], axis=0
    )
    gx[x, 4] = k_end[: T // 2]
    gx[x, 5] = k_end[T // 2 :]

    loads[5].wait()
    val_v[...] = dot(x_v[...], w_v[...]).astype(BF16)
    v = val_v[...]
    span_state = dot_tn(v, k_end.astype(BF16))
    for s in range(NX):
        x1s[1, s, :SLAB, :] = span_state[s * SLAB : (s + 1) * SLAB]
        x1s[1, s, SLAB:, :] = wide_decay
    x_leg(1)

    def slab(i, t):
        return x1r[i, t, :SLAB, :]

    def slab_decay(i, t):
        return x1r[i, t, SLAB : SLAB + 1, :]

    def z_copy(i, t, slot):
        return remote(z2s.at[i], z2r.at[i, slot], sent.at[Z2], z2_rs.at[slot], z_dev(t))

    x_leg_wait(0)
    inner = [None] * NX
    inner[3] = jnp.zeros((SLAB, DK), F32)
    for t in (2, 1, 0):
        inner[t] = slab(0, t + 1) + slab_decay(0, t + 1) * inner[t + 1]
    row_decay = slab_decay(0, 0) * slab_decay(0, 1) * slab_decay(0, 2) * slab_decay(0, 3)
    z2s[0, :SLAB, :] = slab(0, 0) + slab_decay(0, 0) * inner[0]
    z2s[0, SLAB:, :] = jnp.broadcast_to(row_decay, (8, DK))
    for k in (4, 3, 5, 2, 6, 1, 7):
        @pl.when(z >= k)
        def _():
            z_copy(0, z - k, z).start()

    def xi_copy(src, slot, to):
        return remote(xis.at[src], xir.at[slot], sent.at[XI], xi_rs.at[0], x_dev(to))

    for t in range(NX):
        xis[t] = inner[t]
    for k in (2, 1, 3):
        t = lax.rem(x + k, NX)
        xi_copy(t, x, t).start()
    xir[x] = xis[x]
    gx_own(0)

    sibling = tp + 1 - 2 * lax.rem(tp, 2)

    def xy_copy(j, k, slot, to):
        ref = xg.at[slot, k]
        return remote(ref, ref, sent.at[XY], xy_rs.at[j - 1, k], tp_dev(to))

    def xc_copy(k, slot):
        ref = xg.at[slot, k]
        return remote(ref, ref, sent.at[XC], xc_rs.at[0], tp_dev(sibling))

    for k in (1, 3, 2):
        xx_copy(k, lax.rem(x + NX - k, NX)).wait_recv()
        for j in (2, 1, 3):
            xy_copy(j, 3 - k, tp, lax.rem(tp + 2 * j, NT)).start()
        xc_copy(3 - k, tp).start()

    arrived(xir.at[pl.ds(0, 3)], xi_rs.at[0])
    adj_row = xir[...].reshape(DV, DK)
    row_vg = local_vg + dot_nt(k_end.astype(BF16), adj_row.astype(BF16))
    for h in range(2):
        for p in range(2):
            gx[x, 2 * h + p] = row_vg[p * 128 : (p + 1) * 128, h * DK : (h + 1) * DK]
    gx_own(1)
    gx_forward(0)

    def adj_step(n, acc):
        t = NZ - 1 - n
        z_copy(0, t, t).wait_recv()
        return z2r[0, t, :SLAB, :] + z2r[0, t, SLAB : SLAB + 1, :] * acc

    x3s[0, 0] = lax.fori_loop(0, NZ - 1 - z, adj_step, jnp.zeros((SLAB, DK), F32))

    def x3_copy(i, src, slot, to):
        return remote(x3s.at[i, src], x3r.at[i, slot], sent.at[X3 + i], x3_rs.at[i], x_dev(to))

    def x3_wait(i):
        arrived(x3r.at[i, pl.ds(0, 3)], x3_rs.at[i])

    for k in (2, 1, 3):
        x3_copy(0, 0, x, lax.rem(x + k, NX)).start()
    x3r[0, x] = x3s[0, 0]

    gx_forward(1)
    gx_own(2)
    x_leg_wait(1)
    acc = slab(1, 0)
    for t in range(1, NX):
        acc = slab(1, t) + slab_decay(1, t) * acc
    z2s[1, :SLAB, :] = acc
    z2s[1, SLAB:, :] = jnp.broadcast_to(row_decay, (8, DK))
    for k in (4, 3, 5, 2, 6, 1, 7):
        @pl.when(z + k < NZ)
        def _():
            z_copy(1, z + k, z).start()

    for k in (1, 3, 2):
        for j in (1, 3, 2):
            slot = lax.rem(tp + NT - 2 * j, NT)
            xy_copy(j, 3 - k, slot, slot).wait_recv()
            xc_copy(3 - k, slot).start()
    arrived(xg.at[pl.ds(0, 4)], xc_rs.at[0])

    def columns(t):
        return pl.ds(pl.multiple_of(t * T, T), T)

    xb_v[:, :, columns(x)] = xt_v[x]
    for k in range(1, NX):
        xb_v[:, :, columns(lax.rem(x + k, NX))] = xg[:, k - 1].astype(BF16)

    def rz_copy(h, src, slot, to):
        return remote(dwp.at[h, src], rzr.at[h, slot], sent.at[RZ + h], rz_rs.at[h], z_dev(to))

    def product(h, t):
        k_t = gx[t, 4:6].reshape(T, DK).astype(BF16)
        a_t = as_v[t, h * DK : (h + 1) * DK].astype(BF16)
        vg = (gx[t, 2 * h : 2 * h + 2].reshape(T, DK) + dot_nt(k_t, a_t)).astype(BF16)
        return dot(xb_v[:, :, columns(t)].reshape(NZ * ROWS, T), vg)

    def half_product(h):
        gx_wait(gx_rest, h + 1)
        near = product(h, x) + product(h, left) + product(h, right)
        gx_wait(gx_far, h + 1)
        dwp[h] = (near + product(h, far)).reshape(NZ, ROWS, DK)
        for k in (4, 3, 5, 2, 6, 1, 7):
            t = lax.rem(z + k, NZ)
            rz_copy(h, t, z, t).start()

    gx_wait(gx_rest, 0)
    gx_wait(gx_far, 0)
    x3_wait(0)
    acc = x3r[0].reshape(DV, DK)
    for t in (3, 2, 1, 0):
        as_v[t] = acc
        if t:
            acc = slab_decay(0, t) * acc
    half_product(0)
    gx_forward(2)
    half_product(1)
    adj_in = adj_row + as_v[x]
    adj_in16 = adj_in.astype(BF16)

    state = jnp.zeros((DV, DK), F32)
    for b in range(NB):
        sl = slice(b * BLK, (b + 1) * BLK)
        locs_v[b] = state.astype(BF16)
        if b < NB - 1:
            state = jnp.exp(ends[b]) * state + dot_tn(v[sl], tail_k[sl])
    out_dots = jnp.where(lower, dot_nt(do, v), 0.0).astype(BF16)
    out_dots_t = jnp.where(upper, dot_nt(v, do), 0.0).astype(BF16)
    local_qg = dot(out_dots, shrunk_k) + jnp.concatenate(
        [dot(do[b * BLK : (b + 1) * BLK], locs_v[b]) for b in range(NB)], axis=0
    )
    local_kg = exp_nc * dot(out_dots_t, grown_q) + exp_tail * jnp.concatenate(
        [dot(v[b * BLK : (b + 1) * BLK], adjs_v[b]) for b in range(NB)], axis=0
    )
    kg = local_kg + to_end * dot(v, adj_in16)
    dk_v[...] = kg.astype(BF16)

    def state_step(t, acc):
        z_copy(1, t, t).wait_recv()
        return z2r[1, t, :SLAB, :] + z2r[1, t, SLAB : SLAB + 1, :] * acc

    acc = lax.fori_loop(0, z, state_step, jnp.zeros((SLAB, DK), F32))
    for t in range(NX):
        x3s[1, t] = acc
        if t < NX - 1:
            acc = slab(1, t) + slab_decay(1, t) * acc
    for k in (2, 1, 3):
        t = lax.rem(x + k, NX)
        x3_copy(1, t, x, t).start()
    x3r[1, x] = x3s[1, x]
    x3_wait(1)
    state_in = x3r[1].reshape(DV, DK)
    qg = exp_c * local_qg + from_start * dot(do, state_in.astype(BF16))
    dq_v[...] = (qg * (DK**-0.5)).astype(BF16)
    carry = jnp.sum(adj_in * (span_state + span_decay * state_in), axis=0, keepdims=True)
    dg_v[...] = exact_sum((col >= row).astype(BF16), qs * qg - kf * kg) + carry
    stores = [
        pltpu.make_async_copy(src, dst, out_sem.at[i])
        for i, (src, dst) in enumerate(((dq_v, dq_o), (dk_v, dk_o), (dg_v, dg_o), (dwo_v, dwo_o), (rn_v, rn_o)))
    ]
    for store in stores[:3]:
        store.start()

    left_here(x1s.at[0, pl.ds(0, 3)], sent.at[X1])
    left_here(x1s.at[1, pl.ds(0, 3)], sent.at[X1 + 1])
    left_here(z2r.at[0, pl.ds(0, 7)], sent.at[Z2])
    left_here(xis.at[pl.ds(0, 3)], sent.at[XI])
    left_here(x3r.at[0, pl.ds(0, 3)], sent.at[X3])
    left_here(x3r.at[1, pl.ds(0, 3)], sent.at[X3 + 1])
    left_here(gx.at[pl.ds(0, 3)], sent.at[GX])
    left_here(xts.at[pl.ds(0, 3)], sent.at[XX])
    left_here(xg.at[pl.ds(0, 3)], sent.at[XY])
    left_here(xg.at[pl.ds(0, 4)], sent.at[XC])
    for store in stores[:3]:
        store.wait()

    squares = jnp.zeros((ROWS, DK), F32)
    for h in range(2):
        part = dwp[h, z]
        arrived(rzr.at[h, pl.ds(0, 7)], rz_rs.at[h])
        for k in range(1, NZ):
            part = part + rzr[h, lax.rem(z + k, NZ)]
        dwo_v[:, h * DK : (h + 1) * DK] = part
        squares = squares + part * part
    stores[3].start()

    norms = jnp.sum(squares.T, axis=0, keepdims=True)
    tps[...] = jnp.broadcast_to(jnp.concatenate([norms, jnp.zeros((1, 64), F32)], axis=1), (8, 128))

    def tp_copy(slot, to):
        return remote(tps, tpr.at[slot], sent.at[TP], tp_rs.at[0], tp_dev(to))

    for k in range(1, NT):
        tp_copy(tp, lax.rem(tp + k, NT)).start()
    left_here(dwp.at[0, pl.ds(0, 7)], sent.at[RZ])
    left_here(dwp.at[1, pl.ds(0, 7)], sent.at[RZ + 1])
    stores[3].wait()
    left_here(tpr.at[pl.ds(0, 7)], sent.at[TP])
    arrived(tpr.at[pl.ds(0, 7)], tp_rs.at[0])
    acc = tps[0:1, :]
    for k in range(1, NT):
        t = lax.rem(tp + NT - k, NT)
        acc = acc + tpr[t, 0:1, :]
    rn_v[...] = acc[:, :ROWS]
    stores[4].start()
    stores[4].wait()


def finish(*refs):
    ins, outs, sem = refs[:5], refs[5:10], refs[10]
    copies = [pltpu.make_async_copy(src, dst, sem.at[i]) for i, (src, dst) in enumerate(zip(ins, outs))]
    for cp in copies:
        cp.start()
    for cp in copies:
        cp.wait()


def on_device(block_input, queries, keys, w_value, log_decay, d_out):
    dma, vmem = pltpu.SemaphoreType.DMA, pltpu.VMEM
    hbm_spec = pl.BlockSpec(memory_space=pltpu.HBM)
    shapes = (((T, DK), BF16), ((T, DK), BF16), ((T, DK), F32), ((ROWS, DV), F32), ((1, ROWS), F32))
    args = [
        pltpu.with_memory_space_constraint(a, pltpu.HBM)
        for a in (block_input, queries, keys, w_value, log_decay, d_out)
    ]
    outs = pl.pallas_call(
        kernel,
        out_shape=tuple(vmem(*s) for s in shapes),
        in_specs=[hbm_spec] * 6,
        out_specs=(pl.BlockSpec(memory_space=pl.ANY),) * 5,
        scratch_shapes=[
            vmem((T, 2048), BF16), vmem((T, DK), BF16), vmem((T, DK), BF16),
            vmem((2048, DV), BF16), vmem((T, DK), F32), vmem((T, DV), BF16),
            vmem((T, DK), BF16), vmem((T, DK), BF16), vmem((T, DK), F32),
            vmem((ROWS, DV), F32), vmem((1, ROWS), F32),
            vmem((NX, NZ, ROWS, T), BF16), vmem((T, DV), BF16),
            vmem((NB, DV, DK), BF16), vmem((NB, DV, DK), BF16),
            vmem((NX, DV, DK), F32), vmem((NZ, ROWS, NX * T), BF16),
            vmem((2, NX, SLAB + 8, DK), F32), vmem((2, NX, SLAB + 8, DK), F32),
            vmem((2, SLAB + 8, DK), F32), vmem((2, NZ, SLAB + 8, DK), F32),
            vmem((NX, SLAB, DK), F32), vmem((NX, SLAB, DK), F32),
            vmem((2, NX, SLAB, DK), F32), vmem((2, NX, SLAB, DK), F32),
            vmem((NX, 6, T // 2, DK), F32), vmem((NX, ROWS, T), F32), vmem((NT, NX - 1, ROWS, T), F32),
            vmem((2, NZ, ROWS, DK), F32), vmem((2, NZ, ROWS, DK), F32),
            vmem((8, 128), F32), vmem((NT, 8, 128), F32),
            dma((6,)), dma((5,)), dma((13,)), dma((2,)), dma((NZ,)), dma((1,)), dma((2,)), dma((2, 3)), dma((3,)),
            dma((3,)), dma((3,)), dma((3, 3)), dma((1,)), dma((2,)), dma((1,)),
        ],
        compiler_params=pltpu.CompilerParams(collective_id=0, has_side_effects=True, vmem_limit_bytes=40 << 20),
        name="gla_backward",
    )(*args)
    outs = pl.pallas_call(
        finish,
        out_shape=tuple(jax.ShapeDtypeStruct(*s) for s in shapes),
        in_specs=[pl.BlockSpec(memory_space=pl.ANY)] * 5,
        out_specs=(hbm_spec,) * 5,
        scratch_shapes=[dma((5,))],
        compiler_params=pltpu.CompilerParams(vmem_limit_bytes=1 << 20),
        name="finish",
    )(*outs)
    return (*outs[:4], outs[4].reshape(ROWS))


def solution(mesh):
    in_specs = (P("sp", None), P("sp", "tp"), P("sp", "tp"), P(None, "tp"), P("sp", "tp"), P("sp", "tp"))
    out_specs = (P("sp", "tp"), P("sp", "tp"), P("sp", "tp"), P("sp", "tp"), P("sp"))
    return jax.shard_map(on_device, mesh=mesh, in_specs=in_specs, out_specs=out_specs, check_vma=False)
```

```python
import jax
import jax.numpy as jnp
from jax import lax
from jax.experimental import pallas as pl
from jax.experimental.pallas import tpu as pltpu
from jax.sharding import PartitionSpec as P

DK = 128
DV = 256
T = 256
BLK = 32
NB = T // BLK
NZ, NX, NT = 8, 4, 8
SLAB = DV // NX
ROWS = 64
X1, Z2, XI, X3, GX, XX, XY, XC, RZ, TP = 0, 2, 3, 4, 6, 7, 8, 9, 10, 12
MESH = pl.DeviceIdType.MESH
F32, BF16 = jnp.float32, jnp.bfloat16


def dot(a, b):
    return jnp.dot(a, b, preferred_element_type=F32)


def dot_nt(a, b):
    return lax.dot_general(a, b, (((1,), (1,)), ((), ())), preferred_element_type=F32)


def dot_tn(a, b):
    return lax.dot_general(a, b, (((0,), (0,)), ((), ())), preferred_element_type=F32)


def exact_sum(ones, a):
    hi = a.astype(BF16)
    rest = a - hi.astype(F32)
    mid = rest.astype(BF16)
    low = (rest - mid.astype(F32)).astype(BF16)
    return dot(ones, hi) + (dot(ones, mid) + dot(ones, low))


def kernel(
    x_hbm, q_hbm, k_hbm, w_hbm, g_hbm, do_hbm,
    dq_o, dk_o, dg_o, dwo_o, rn_o,
    x_v, q_v, k_v, w_v, g_v, do_v, dq_v, dk_v, dg_v, dwo_v, rn_v,
    xt_v, val_v, locs_v, adjs_v, as_v, xb_v,
    x1s, x1r, z2s, z2r, xis, xir, x3s, x3r, gx, xts, xg, dwp, rzr, tps, tpr,
    in_sem, out_sem, sent, x1_rs, z2_rs, xi_rs, x3_rs, gx_rs, gx_rest, gx_far, xx_rs, xy_rs, xc_rs, rz_rs, tp_rs,
):
    sp, tp = lax.axis_index("sp"), lax.axis_index("tp")
    z, x = sp // NX, lax.rem(sp, NX)

    def x_dev(t):
        return {"sp": z * NX + t}

    def z_dev(t):
        return {"sp": t * NX + x}

    def tp_dev(t):
        return {"tp": t}

    loads = [
        pltpu.make_async_copy(src, dst, in_sem.at[i])
        for i, (src, dst) in enumerate(
            ((g_hbm, g_v), (q_hbm, q_v), (do_hbm, do_v), (k_hbm, k_v), (x_hbm, x_v), (w_hbm, w_v))
        )
    ]
    for load in loads[:3]:
        load.start()

    barrier = pltpu.get_barrier_semaphore()
    for k in (4, 3, 5, 2, 6, 1, 7):
        pl.semaphore_signal(barrier, inc=1, device_id=z_dev(lax.rem(z + k, NZ)), device_id_type=MESH)
    for k in (2, 1, 3):
        pl.semaphore_signal(barrier, inc=1, device_id=x_dev(lax.rem(x + k, NX)), device_id_type=MESH)
    for k in range(1, NT):
        pl.semaphore_signal(barrier, inc=1, device_id=tp_dev(lax.rem(tp + k, NT)), device_id_type=MESH)
    for load in loads[3:]:
        load.start()

    def remote(src, dst, ss, rs, dev):
        return pltpu.make_async_remote_copy(
            src_ref=src, dst_ref=dst, send_sem=ss, recv_sem=rs, device_id=dev, device_id_type=MESH
        )

    row = lax.broadcasted_iota(jnp.int32, (T, T), 0)
    col = lax.broadcasted_iota(jnp.int32, (T, T), 1)
    same = (row >> 5) == (col >> 5)
    lower = same & (col <= row)
    upper = same & (col >= row)

    loads[0].wait()
    c = exact_sum(lower.astype(BF16), g_v[...])
    c3 = c.reshape(NB, BLK, DK)
    ends = [c3[b, BLK - 1 : BLK, :] for b in range(NB)]
    before = [jnp.zeros((1, DK), F32)]
    for b in range(NB):
        before.append(before[-1] + ends[b])
    after = [jnp.zeros((1, DK), F32)]
    for b in reversed(range(1, NB)):
        after.append(after[-1] + ends[b])
    after = after[::-1]
    total = before[NB]

    def per_block(rows):
        return jnp.concatenate([jnp.broadcast_to(r, (BLK, DK)) for r in rows], axis=0)

    end_wide = per_block(ends)
    from_start = jnp.exp(c + per_block(before[:NB]))
    tail_log = end_wide - c
    to_end = jnp.exp(tail_log + per_block(after))
    span_decay = jnp.exp(total)

    loads[1].wait()
    loads[2].wait()
    qs = q_v[...].astype(F32) * (DK**-0.5)
    do = do_v[...]
    span_adj = dot_tn(do, (qs * from_start).astype(BF16))
    wide_decay = jnp.broadcast_to(span_decay, (8, DK))
    for s in range(NX):
        x1s[0, s, :SLAB, :] = span_adj[s * SLAB : (s + 1) * SLAB]
        x1s[0, s, SLAB:, :] = wide_decay

    pl.semaphore_wait(barrier, NX - 1 + NZ - 1 + NT - 1)

    def x1_copy(i, src, slot, to):
        rows = pl.ds(0, SLAB + 8 * (1 - i))
        return remote(x1s.at[i, src, rows], x1r.at[i, slot, rows], sent.at[X1 + i], x1_rs.at[i], x_dev(to))

    def x_leg(i):
        for k in (2, 1, 3):
            t = lax.rem(x + k, NX)
            x1_copy(i, t, x, t).start()
        x1r[i, x] = x1s[i, x]

    def arrived(ref, sem):
        remote(ref, ref, sent.at[0], sem, x_dev(x)).wait_recv()

    def left_here(ref, sem):
        remote(ref, ref, sem, x1_rs.at[0], x_dev(x)).wait_send()

    def x_leg_wait(i):
        arrived(x1r.at[i, pl.ds(0, 3), pl.ds(0, SLAB + 8 * (1 - i))], x1_rs.at[i])

    x_leg(0)

    loads[4].wait()
    for zz in range(NZ):
        xt_v[:, zz] = x_v[:, zz * NX * ROWS : (zz + 1) * NX * ROWS].T.reshape(NX, ROWS, T)
    for t in range(NX):
        xts[t] = xt_v[t, tp].astype(F32)

    def xx_copy(k, t):
        return remote(xts.at[t], xg.at[tp, 3 - k], sent.at[XX], xx_rs.at[k - 1], x_dev(t))

    for k in (1, 3, 2):
        xx_copy(k, lax.rem(x + k, NX)).start()

    right, left, far = lax.rem(x + 1, NX), lax.rem(x + 3, NX), lax.rem(x + 2, NX)
    ways = (right, left, right, left)

    def gx_copy(kind, piece, slot, sem, rows):
        ref = gx.at[slot, piece, rows]
        return remote(ref, ref, sent.at[GX], sem, x_dev(ways[kind]))

    stages = ((4, 5), (0, 1), (2, 3))

    def cuts(stage):
        n = 2 if stage == 2 else 1
        return [(stage + i, pl.ds(i * (T // 2 // n), T // 2 // n)) for i in range(n)]

    def gx_own(stage):
        a, b = stages[stage]
        for n, rows in cuts(stage):
            gx_copy(0, a, x, gx_rs.at[0, n], rows).start()
            gx_copy(1, b, x, gx_rs.at[1, n], rows).start()
        whole = pl.ds(0, T // 2)
        gx_copy(0, b, x, gx_rest.at[stage], whole).start()
        gx_copy(1, a, x, gx_rest.at[stage], whole).start()

    def gx_forward(stage):
        a, b = stages[stage]
        for n, rows in cuts(stage):
            gx_copy(0, a, left, gx_rs.at[0, n], rows).wait_recv()
            gx_copy(2, a, left, gx_far.at[stage], rows).start()
            gx_copy(1, b, right, gx_rs.at[1, n], rows).wait_recv()
            gx_copy(3, b, right, gx_far.at[stage], rows).start()

    def gx_wait(sems, stage):
        arrived(gx.at[0, pl.ds(0, 2)], sems.at[stage])

    loads[3].wait()
    kf = k_v[...].astype(F32)
    exp_c = jnp.exp(c)
    exp_nc = jnp.exp(-c)
    exp_tail = jnp.exp(tail_log)
    grown_q = (qs * exp_c).astype(BF16)
    shrunk_k = (kf * exp_nc).astype(BF16)
    tail_k = (kf * exp_tail).astype(BF16)
    k_end = kf * to_end
    adj = jnp.zeros((DV, DK), F32)
    for b in reversed(range(NB)):
        sl = slice(b * BLK, (b + 1) * BLK)
        adjs_v[b] = adj.astype(BF16)
        if b:
            adj = jnp.exp(ends[b]) * adj + dot_tn(do[sl], grown_q[sl])
    key_dots_t = jnp.where(upper, dot_nt(shrunk_k, grown_q), 0.0).astype(BF16)
    local_vg = dot(key_dots_t, do) + jnp.concatenate(
        [dot_nt(tail_k[b * BLK : (b + 1) * BLK], adjs_v[b]) for b in range(NB)], axis=0
    )
    gx[x, 4] = k_end[: T // 2]
    gx[x, 5] = k_end[T // 2 :]

    loads[5].wait()
    val_v[...] = dot(x_v[...], w_v[...]).astype(BF16)
    v = val_v[...]
    span_state = dot_tn(v, k_end.astype(BF16))
    for s in range(NX):
        x1s[1, s, :SLAB, :] = span_state[s * SLAB : (s + 1) * SLAB]
        x1s[1, s, SLAB:, :] = wide_decay
    x_leg(1)

    def slab(i, t):
        return x1r[i, t, :SLAB, :]

    def slab_decay(i, t):
        return x1r[i, t, SLAB : SLAB + 1, :]

    def z_copy(i, t, slot):
        return remote(z2s.at[i], z2r.at[i, slot], sent.at[Z2], z2_rs.at[slot], z_dev(t))

    x_leg_wait(0)
    inner = [None] * NX
    inner[3] = jnp.zeros((SLAB, DK), F32)
    for t in (2, 1, 0):
        inner[t] = slab(0, t + 1) + slab_decay(0, t + 1) * inner[t + 1]
    row_decay = slab_decay(0, 0) * slab_decay(0, 1) * slab_decay(0, 2) * slab_decay(0, 3)
    z2s[0, :SLAB, :] = slab(0, 0) + slab_decay(0, 0) * inner[0]
    z2s[0, SLAB:, :] = jnp.broadcast_to(row_decay, (8, DK))
    for k in (4, 3, 5, 2, 6, 1, 7):
        @pl.when(z >= k)
        def _():
            z_copy(0, z - k, z).start()

    def xi_copy(src, slot, to):
        return remote(xis.at[src], xir.at[slot], sent.at[XI], xi_rs.at[0], x_dev(to))

    for t in range(NX):
        xis[t] = inner[t]
    for k in (2, 1, 3):
        t = lax.rem(x + k, NX)
        xi_copy(t, x, t).start()
    xir[x] = xis[x]
    gx_own(0)

    sibling = tp + 1 - 2 * lax.rem(tp, 2)

    def xy_copy(j, k, slot, to):
        ref = xg.at[slot, k]
        return remote(ref, ref, sent.at[XY], xy_rs.at[j - 1, k], tp_dev(to))

    def xc_copy(k, slot):
        ref = xg.at[slot, k]
        return remote(ref, ref, sent.at[XC], xc_rs.at[0], tp_dev(sibling))

    for k in (1, 3, 2):
        xx_copy(k, lax.rem(x + NX - k, NX)).wait_recv()
        for j in (2, 1, 3):
            xy_copy(j, 3 - k, tp, lax.rem(tp + 2 * j, NT)).start()
        xc_copy(3 - k, tp).start()

    arrived(xir.at[pl.ds(0, 3)], xi_rs.at[0])
    adj_row = xir[...].reshape(DV, DK)
    row_vg = local_vg + dot_nt(k_end.astype(BF16), adj_row.astype(BF16))
    for h in range(2):
        for p in range(2):
            gx[x, 2 * h + p] = row_vg[p * 128 : (p + 1) * 128, h * DK : (h + 1) * DK]
    gx_own(1)
    gx_forward(0)

    def adj_step(n, acc):
        t = NZ - 1 - n
        z_copy(0, t, t).wait_recv()
        return z2r[0, t, :SLAB, :] + z2r[0, t, SLAB : SLAB + 1, :] * acc

    x3s[0, 0] = lax.fori_loop(0, NZ - 1 - z, adj_step, jnp.zeros((SLAB, DK), F32))

    def x3_copy(i, src, slot, to):
        return remote(x3s.at[i, src], x3r.at[i, slot], sent.at[X3 + i], x3_rs.at[i], x_dev(to))

    def x3_wait(i):
        arrived(x3r.at[i, pl.ds(0, 3)], x3_rs.at[i])

    for k in (2, 1, 3):
        x3_copy(0, 0, x, lax.rem(x + k, NX)).start()
    x3r[0, x] = x3s[0, 0]

    gx_forward(1)
    gx_own(2)
    x_leg_wait(1)
    acc = slab(1, 0)
    for t in range(1, NX):
        acc = slab(1, t) + slab_decay(0, t) * acc
    z2s[1, :SLAB, :] = acc
    z2s[1, SLAB:, :] = jnp.broadcast_to(row_decay, (8, DK))
    for k in (4, 3, 5, 2, 6, 1, 7):
        @pl.when(z + k < NZ)
        def _():
            z_copy(1, z + k, z).start()

    for k in (1, 3, 2):
        for j in (1, 3, 2):
            slot = lax.rem(tp + NT - 2 * j, NT)
            xy_copy(j, 3 - k, slot, slot).wait_recv()
            xc_copy(3 - k, slot).start()
    arrived(xg.at[pl.ds(0, 4)], xc_rs.at[0])

    def columns(t):
        return pl.ds(pl.multiple_of(t * T, T), T)

    xb_v[:, :, columns(x)] = xt_v[x]
    for k in range(1, NX):
        xb_v[:, :, columns(lax.rem(x + k, NX))] = xg[:, k - 1].astype(BF16)

    def rz_copy(h, src, slot, to):
        return remote(dwp.at[h, src], rzr.at[h, slot], sent.at[RZ + h], rz_rs.at[h], z_dev(to))

    def product(h, t):
        k_t = gx[t, 4:6].reshape(T, DK).astype(BF16)
        a_t = as_v[t, h * DK : (h + 1) * DK].astype(BF16)
        vg = (gx[t, 2 * h : 2 * h + 2].reshape(T, DK) + dot_nt(k_t, a_t)).astype(BF16)
        return dot(xb_v[:, :, columns(t)].reshape(NZ * ROWS, T), vg)

    def half_product(h):
        gx_wait(gx_rest, h + 1)
        near = product(h, x) + product(h, left) + product(h, right)
        gx_wait(gx_far, h + 1)
        dwp[h] = (near + product(h, far)).reshape(NZ, ROWS, DK)
        for k in (4, 3, 5, 2, 6, 1, 7):
            t = lax.rem(z + k, NZ)
            rz_copy(h, t, z, t).start()

    gx_wait(gx_rest, 0)
    gx_wait(gx_far, 0)
    x3_wait(0)
    acc = x3r[0].reshape(DV, DK)
    for t in (3, 2, 1, 0):
        as_v[t] = acc
        if t:
            acc = slab_decay(0, t) * acc
    half_product(0)
    gx_forward(2)
    half_product(1)
    adj_in = adj_row + as_v[x]
    adj_in16 = adj_in.astype(BF16)

    state = jnp.zeros((DV, DK), F32)
    for b in range(NB):
        sl = slice(b * BLK, (b + 1) * BLK)
        locs_v[b] = state.astype(BF16)
        if b < NB - 1:
            state = jnp.exp(ends[b]) * state + dot_tn(v[sl], tail_k[sl])
    out_dots = jnp.where(lower, dot_nt(do, v), 0.0).astype(BF16)
    out_dots_t = jnp.where(upper, dot_nt(v, do), 0.0).astype(BF16)
    local_qg = dot(out_dots, shrunk_k) + jnp.concatenate(
        [dot(do[b * BLK : (b + 1) * BLK], locs_v[b]) for b in range(NB)], axis=0
    )
    local_kg = exp_nc * dot(out_dots_t, grown_q) + exp_tail * jnp.concatenate(
        [dot(v[b * BLK : (b + 1) * BLK], adjs_v[b]) for b in range(NB)], axis=0
    )
    kg = local_kg + to_end * dot(v, adj_in16)
    dk_v[...] = kg.astype(BF16)

    def state_step(t, acc):
        z_copy(1, t, t).wait_recv()
        return z2r[1, t, :SLAB, :] + z2r[1, t, SLAB : SLAB + 1, :] * acc

    acc = lax.fori_loop(0, z, state_step, jnp.zeros((SLAB, DK), F32))
    for t in range(NX):
        x3s[1, t] = acc
        if t < NX - 1:
            acc = slab(1, t) + slab_decay(0, t) * acc
    for k in (2, 1, 3):
        t = lax.rem(x + k, NX)
        x3_copy(1, t, x, t).start()
    x3r[1, x] = x3s[1, x]
    x3_wait(1)
    state_in = x3r[1].reshape(DV, DK)
    qg = exp_c * local_qg + from_start * dot(do, state_in.astype(BF16))
    dq_v[...] = (qg * (DK**-0.5)).astype(BF16)
    carry = jnp.sum(adj_in * (span_state + span_decay * state_in), axis=0, keepdims=True)
    dg_v[...] = exact_sum((col >= row).astype(BF16), qs * qg - kf * kg) + carry
    stores = [
        pltpu.make_async_copy(src, dst, out_sem.at[i])
        for i, (src, dst) in enumerate(((dq_v, dq_o), (dk_v, dk_o), (dg_v, dg_o), (dwo_v, dwo_o), (rn_v, rn_o)))
    ]
    for store in stores[:3]:
        store.start()

    left_here(x1s.at[0, pl.ds(0, 3)], sent.at[X1])
    left_here(x1s.at[1, pl.ds(0, 3), pl.ds(0, SLAB)], sent.at[X1 + 1])
    left_here(z2r.at[0, pl.ds(0, 7)], sent.at[Z2])
    left_here(xis.at[pl.ds(0, 3)], sent.at[XI])
    left_here(x3r.at[0, pl.ds(0, 3)], sent.at[X3])
    left_here(x3r.at[1, pl.ds(0, 3)], sent.at[X3 + 1])
    left_here(gx.at[pl.ds(0, 3)], sent.at[GX])
    left_here(xts.at[pl.ds(0, 3)], sent.at[XX])
    left_here(xg.at[pl.ds(0, 3)], sent.at[XY])
    left_here(xg.at[pl.ds(0, 4)], sent.at[XC])
    for store in stores[:3]:
        store.wait()

    squares = jnp.zeros((ROWS, DK), F32)
    for h in range(2):
        part = dwp[h, z]
        arrived(rzr.at[h, pl.ds(0, 7)], rz_rs.at[h])
        for k in range(1, NZ):
            part = part + rzr[h, lax.rem(z + k, NZ)]
        dwo_v[:, h * DK : (h + 1) * DK] = part
        squares = squares + part * part
    stores[3].start()

    norms = jnp.sum(squares.T, axis=0, keepdims=True)
    tps[...] = jnp.broadcast_to(jnp.concatenate([norms, jnp.zeros((1, 64), F32)], axis=1), (8, 128))

    def tp_copy(slot, to):
        return remote(tps, tpr.at[slot], sent.at[TP], tp_rs.at[0], tp_dev(to))

    for k in range(1, NT):
        tp_copy(tp, lax.rem(tp + k, NT)).start()
    left_here(dwp.at[0, pl.ds(0, 7)], sent.at[RZ])
    left_here(dwp.at[1, pl.ds(0, 7)], sent.at[RZ + 1])
    stores[3].wait()
    left_here(tpr.at[pl.ds(0, 7)], sent.at[TP])
    arrived(tpr.at[pl.ds(0, 7)], tp_rs.at[0])
    acc = tps[0:1, :]
    for k in range(1, NT):
        t = lax.rem(tp + NT - k, NT)
        acc = acc + tpr[t, 0:1, :]
    rn_v[...] = acc[:, :ROWS]
    stores[4].start()
    stores[4].wait()


def finish(*refs):
    ins, outs, sem = refs[:5], refs[5:10], refs[10]
    copies = [pltpu.make_async_copy(src, dst, sem.at[i]) for i, (src, dst) in enumerate(zip(ins, outs))]
    for cp in copies:
        cp.start()
    for cp in copies:
        cp.wait()


def on_device(block_input, queries, keys, w_value, log_decay, d_out):
    dma, vmem = pltpu.SemaphoreType.DMA, pltpu.VMEM
    hbm_spec = pl.BlockSpec(memory_space=pltpu.HBM)
    shapes = (((T, DK), BF16), ((T, DK), BF16), ((T, DK), F32), ((ROWS, DV), F32), ((1, ROWS), F32))
    args = [
        pltpu.with_memory_space_constraint(a, pltpu.HBM)
        for a in (block_input, queries, keys, w_value, log_decay, d_out)
    ]
    outs = pl.pallas_call(
        kernel,
        out_shape=tuple(vmem(*s) for s in shapes),
        in_specs=[hbm_spec] * 6,
        out_specs=(pl.BlockSpec(memory_space=pl.ANY),) * 5,
        scratch_shapes=[
            vmem((T, 2048), BF16), vmem((T, DK), BF16), vmem((T, DK), BF16),
            vmem((2048, DV), BF16), vmem((T, DK), F32), vmem((T, DV), BF16),
            vmem((T, DK), BF16), vmem((T, DK), BF16), vmem((T, DK), F32),
            vmem((ROWS, DV), F32), vmem((1, ROWS), F32),
            vmem((NX, NZ, ROWS, T), BF16), vmem((T, DV), BF16),
            vmem((NB, DV, DK), BF16), vmem((NB, DV, DK), BF16),
            vmem((NX, DV, DK), F32), vmem((NZ, ROWS, NX * T), BF16),
            vmem((2, NX, SLAB + 8, DK), F32), vmem((2, NX, SLAB + 8, DK), F32),
            vmem((2, SLAB + 8, DK), F32), vmem((2, NZ, SLAB + 8, DK), F32),
            vmem((NX, SLAB, DK), F32), vmem((NX, SLAB, DK), F32),
            vmem((2, NX, SLAB, DK), F32), vmem((2, NX, SLAB, DK), F32),
            vmem((NX, 6, T // 2, DK), F32), vmem((NX, ROWS, T), F32), vmem((NT, NX - 1, ROWS, T), F32),
            vmem((2, NZ, ROWS, DK), F32), vmem((2, NZ, ROWS, DK), F32),
            vmem((8, 128), F32), vmem((NT, 8, 128), F32),
            dma((6,)), dma((5,)), dma((13,)), dma((2,)), dma((NZ,)), dma((1,)), dma((2,)), dma((2, 4)), dma((3,)),
            dma((3,)), dma((3,)), dma((3, 3)), dma((1,)), dma((2,)), dma((1,)),
        ],
        compiler_params=pltpu.CompilerParams(collective_id=0, has_side_effects=True, vmem_limit_bytes=40 << 20),
        name="gla_backward",
    )(*args)
    outs = pl.pallas_call(
        finish,
        out_shape=tuple(jax.ShapeDtypeStruct(*s) for s in shapes),
        in_specs=[pl.BlockSpec(memory_space=pl.ANY)] * 5,
        out_specs=(hbm_spec,) * 5,
        scratch_shapes=[dma((5,))],
        compiler_params=pltpu.CompilerParams(vmem_limit_bytes=1 << 20),
        name="finish",
    )(*outs)
    return (*outs[:4], outs[4].reshape(ROWS))


def solution(mesh):
    in_specs = (P("sp", None), P("sp", "tp"), P("sp", "tp"), P(None, "tp"), P("sp", "tp"), P("sp", "tp"))
    out_specs = (P("sp", "tp"), P("sp", "tp"), P("sp", "tp"), P("sp", "tp"), P("sp"))
    return jax.shard_map(on_device, mesh=mesh, in_specs=in_specs, out_specs=out_specs, check_vma=False)
```

```python
import jax
import jax.numpy as jnp
from jax import lax
from jax.experimental import pallas as pl
from jax.experimental.pallas import tpu as pltpu
from jax.sharding import PartitionSpec as P

DK = 128
DV = 256
T = 256
BLK = 32
NB = T // BLK
NZ, NX, NT = 8, 4, 8
SLAB = DV // NX
ROWS = 64
X1, Z2, XI, X3, GX, XX, RZ, TP = 0, 2, 3, 4, 6, 7, 8, 10
MESH = pl.DeviceIdType.MESH
F32, BF16 = jnp.float32, jnp.bfloat16


def dot(a, b):
    return jnp.dot(a, b, preferred_element_type=F32)


def dot_nt(a, b):
    return lax.dot_general(a, b, (((1,), (1,)), ((), ())), preferred_element_type=F32)


def dot_tn(a, b):
    return lax.dot_general(a, b, (((0,), (0,)), ((), ())), preferred_element_type=F32)


def exact_sum(ones, a):
    hi = a.astype(BF16)
    rest = a - hi.astype(F32)
    mid = rest.astype(BF16)
    low = (rest - mid.astype(F32)).astype(BF16)
    return dot(ones, hi) + (dot(ones, mid) + dot(ones, low))


def kernel(
    x_hbm, q_hbm, k_hbm, w_hbm, g_hbm, do_hbm,
    dq_o, dk_o, dg_o, dwo_o, rn_o,
    x_v, q_v, k_v, w_v, g_v, do_v, dq_v, dk_v, dg_v, dwo_v, rn_v,
    xt_v, val_v, locs_v, adjs_v, as_v, xb_v,
    x1s, x1r, z2s, z2r, xis, xir, x3s, x3r, gx, xts, xg, dwp, rzr, tps, tpr,
    in_sem, out_sem, sent, x1_rs, z2_rs, xi_rs, x3_rs, gx_rs, gx_rest, gx_far, xx_rs, xy_rs, xc_rs, rz_rs, tp_rs,
):
    sp, tp = lax.axis_index("sp"), lax.axis_index("tp")
    z, x = sp // NX, lax.rem(sp, NX)

    def x_dev(t):
        return {"sp": z * NX + t}

    def z_dev(t):
        return {"sp": t * NX + x}

    def tp_dev(t):
        return {"tp": t}

    loads = [
        pltpu.make_async_copy(src, dst, in_sem.at[i])
        for i, (src, dst) in enumerate(
            ((g_hbm, g_v), (q_hbm, q_v), (do_hbm, do_v), (k_hbm, k_v), (x_hbm, x_v), (w_hbm, w_v))
        )
    ]
    for load in loads[:3]:
        load.start()

    barrier = pltpu.get_barrier_semaphore()
    for k in (4, 3, 5, 2, 6, 1, 7):
        pl.semaphore_signal(barrier, inc=1, device_id=z_dev(lax.rem(z + k, NZ)), device_id_type=MESH)
    for k in (2, 1, 3):
        pl.semaphore_signal(barrier, inc=1, device_id=x_dev(lax.rem(x + k, NX)), device_id_type=MESH)
    for k in range(1, NT):
        pl.semaphore_signal(barrier, inc=1, device_id=tp_dev(lax.rem(tp + k, NT)), device_id_type=MESH)
    for load in loads[3:]:
        load.start()

    def remote(src, dst, ss, rs, dev):
        return pltpu.make_async_remote_copy(
            src_ref=src, dst_ref=dst, send_sem=ss, recv_sem=rs, device_id=dev, device_id_type=MESH
        )

    row = lax.broadcasted_iota(jnp.int32, (T, T), 0)
    col = lax.broadcasted_iota(jnp.int32, (T, T), 1)
    same = (row >> 5) == (col >> 5)
    lower = same & (col <= row)
    upper = same & (col >= row)

    loads[0].wait()
    c = exact_sum(lower.astype(BF16), g_v[...])
    c3 = c.reshape(NB, BLK, DK)
    ends = [c3[b, BLK - 1 : BLK, :] for b in range(NB)]
    before = [jnp.zeros((1, DK), F32)]
    for b in range(NB):
        before.append(before[-1] + ends[b])
    after = [jnp.zeros((1, DK), F32)]
    for b in reversed(range(1, NB)):
        after.append(after[-1] + ends[b])
    after = after[::-1]
    total = before[NB]

    def per_block(rows):
        return jnp.concatenate([jnp.broadcast_to(r, (BLK, DK)) for r in rows], axis=0)

    end_wide = per_block(ends)
    from_start = jnp.exp(c + per_block(before[:NB]))
    tail_log = end_wide - c
    to_end = jnp.exp(tail_log + per_block(after))
    span_decay = jnp.exp(total)

    loads[1].wait()
    loads[2].wait()
    qs = q_v[...].astype(F32) * (DK**-0.5)
    do = do_v[...]
    span_adj = dot_tn(do, (qs * from_start).astype(BF16))
    wide_decay = jnp.broadcast_to(span_decay, (8, DK))
    for s in range(NX):
        x1s[0, s, :SLAB, :] = span_adj[s * SLAB : (s + 1) * SLAB]
        x1s[0, s, SLAB:, :] = wide_decay

    pl.semaphore_wait(barrier, NX - 1 + NZ - 1 + NT - 1)

    def x1_copy(i, src, slot, to):
        rows = pl.ds(0, SLAB + 8 * (1 - i))
        return remote(x1s.at[i, src, rows], x1r.at[i, slot, rows], sent.at[X1 + i], x1_rs.at[i], x_dev(to))

    def x_leg(i):
        for k in (2, 1, 3):
            t = lax.rem(x + k, NX)
            x1_copy(i, t, x, t).start()
        x1r[i, x] = x1s[i, x]

    def arrived(ref, sem):
        remote(ref, ref, sent.at[0], sem, x_dev(x)).wait_recv()

    def left_here(ref, sem):
        remote(ref, ref, sem, x1_rs.at[0], x_dev(x)).wait_send()

    def x_leg_wait(i):
        arrived(x1r.at[i, pl.ds(0, 3), pl.ds(0, SLAB + 8 * (1 - i))], x1_rs.at[i])

    x_leg(0)

    loads[4].wait()
    for zz in range(NZ):
        xt_v[:, zz] = x_v[:, zz * NX * ROWS : (zz + 1) * NX * ROWS].T.reshape(NX, ROWS, T)
    for t in range(NX):
        xts[t] = xt_v[t, tp].astype(F32)

    def xx_copy(k, t):
        return remote(xts.at[t], xg.at[tp, 3 - k], sent.at[XX], xx_rs.at[k - 1], x_dev(t))

    for k in (1, 3, 2):
        xx_copy(k, lax.rem(x + k, NX)).start()

    right, left, far = lax.rem(x + 1, NX), lax.rem(x + 3, NX), lax.rem(x + 2, NX)
    ways = (right, left, right, left)

    def gx_copy(kind, piece, slot, sem, rows):
        ref = gx.at[slot, piece, rows]
        return remote(ref, ref, sent.at[GX], sem, x_dev(ways[kind]))

    stages = ((4, 5), (0, 1), (2, 3))

    def cuts(stage):
        n = 2 if stage == 2 else 1
        return [(stage + i, pl.ds(i * (T // 2 // n), T // 2 // n)) for i in range(n)]

    def gx_own(stage):
        a, b = stages[stage]
        for n, rows in cuts(stage):
            gx_copy(0, a, x, gx_rs.at[0, n], rows).start()
            gx_copy(1, b, x, gx_rs.at[1, n], rows).start()
        whole = pl.ds(0, T // 2)
        gx_copy(0, b, x, gx_rest.at[stage], whole).start()
        gx_copy(1, a, x, gx_rest.at[stage], whole).start()

    def gx_forward(stage):
        a, b = stages[stage]
        for n, rows in cuts(stage):
            gx_copy(0, a, left, gx_rs.at[0, n], rows).wait_recv()
            gx_copy(2, a, left, gx_far.at[stage], rows).start()
            gx_copy(1, b, right, gx_rs.at[1, n], rows).wait_recv()
            gx_copy(3, b, right, gx_far.at[stage], rows).start()

    def gx_wait(sems, stage):
        arrived(gx.at[0, pl.ds(0, 2)], sems.at[stage])

    loads[3].wait()
    kf = k_v[...].astype(F32)
    exp_c = jnp.exp(c)
    exp_nc = jnp.exp(-c)
    exp_tail = jnp.exp(tail_log)
    grown_q = (qs * exp_c).astype(BF16)
    shrunk_k = (kf * exp_nc).astype(BF16)
    tail_k = (kf * exp_tail).astype(BF16)
    k_end = kf * to_end
    adj = jnp.zeros((DV, DK), F32)
    for b in reversed(range(NB)):
        sl = slice(b * BLK, (b + 1) * BLK)
        adjs_v[b] = adj.astype(BF16)
        if b:
            adj = jnp.exp(ends[b]) * adj + dot_tn(do[sl], grown_q[sl])
    key_dots_t = jnp.where(upper, dot_nt(shrunk_k, grown_q), 0.0).astype(BF16)
    local_vg = dot(key_dots_t, do) + jnp.concatenate(
        [dot_nt(tail_k[b * BLK : (b + 1) * BLK], adjs_v[b]) for b in range(NB)], axis=0
    )
    gx[x, 4] = k_end[: T // 2]
    gx[x, 5] = k_end[T // 2 :]

    loads[5].wait()
    val_v[...] = dot(x_v[...], w_v[...]).astype(BF16)
    v = val_v[...]
    span_state = dot_tn(v, k_end.astype(BF16))
    for s in range(NX):
        x1s[1, s, :SLAB, :] = span_state[s * SLAB : (s + 1) * SLAB]
        x1s[1, s, SLAB:, :] = wide_decay
    x_leg(1)

    def slab(i, t):
        return x1r[i, t, :SLAB, :]

    def slab_decay(i, t):
        return x1r[i, t, SLAB : SLAB + 1, :]

    def z_copy(i, t, slot):
        return remote(z2s.at[i], z2r.at[i, slot], sent.at[Z2], z2_rs.at[slot], z_dev(t))

    x_leg_wait(0)
    inner = [None] * NX
    inner[3] = jnp.zeros((SLAB, DK), F32)
    for t in (2, 1, 0):
        inner[t] = slab(0, t + 1) + slab_decay(0, t + 1) * inner[t + 1]
    row_decay = slab_decay(0, 0) * slab_decay(0, 1) * slab_decay(0, 2) * slab_decay(0, 3)
    z2s[0, :SLAB, :] = slab(0, 0) + slab_decay(0, 0) * inner[0]
    z2s[0, SLAB:, :] = jnp.broadcast_to(row_decay, (8, DK))
    for k in (4, 3, 5, 2, 6, 1, 7):
        @pl.when(z >= k)
        def _():
            z_copy(0, z - k, z).start()

    def xi_copy(src, slot, to):
        return remote(xis.at[src], xir.at[slot], sent.at[XI], xi_rs.at[0], x_dev(to))

    for t in range(NX):
        xis[t] = inner[t]
    for k in (2, 1, 3):
        t = lax.rem(x + k, NX)
        xi_copy(t, x, t).start()
    xir[x] = xis[x]
    gx_own(0)

    sibling = tp + 1 - 2 * lax.rem(tp, 2)

    def xy_copy(j, k, slot, to):
        ref = xg.at[slot, k]
        return remote(ref, ref, sent.at[XX], xy_rs.at[j - 1, k], tp_dev(to))

    def xc_copy(k, slot):
        ref = xg.at[slot, k]
        return remote(ref, ref, sent.at[XX], xc_rs.at[0], tp_dev(sibling))

    for k in (1, 3, 2):
        xx_copy(k, lax.rem(x + NX - k, NX)).wait_recv()
        for j in (2, 1, 3):
            xy_copy(j, 3 - k, tp, lax.rem(tp + 2 * j, NT)).start()
        xc_copy(3 - k, tp).start()

    x_leg_wait(1)
    acc = slab(1, 0)
    for t in range(1, NX):
        acc = slab(1, t) + slab_decay(0, t) * acc
    z2s[1, :SLAB, :] = acc
    z2s[1, SLAB:, :] = jnp.broadcast_to(row_decay, (8, DK))
    for k in (4, 3, 5, 2, 6, 1, 7):
        @pl.when(z + k < NZ)
        def _():
            z_copy(1, z + k, z).start()

    arrived(xir.at[pl.ds(0, 3)], xi_rs.at[0])
    adj_row = xir[...].reshape(DV, DK)
    row_vg = local_vg + dot_nt(k_end.astype(BF16), adj_row.astype(BF16))
    for h in range(2):
        for p in range(2):
            gx[x, 2 * h + p] = row_vg[p * 128 : (p + 1) * 128, h * DK : (h + 1) * DK]
    gx_own(1)
    gx_forward(0)

    def adj_step(n, acc):
        t = NZ - 1 - n
        z_copy(0, t, t).wait_recv()
        return z2r[0, t, :SLAB, :] + z2r[0, t, SLAB : SLAB + 1, :] * acc

    x3s[0, 0] = lax.fori_loop(0, NZ - 1 - z, adj_step, jnp.zeros((SLAB, DK), F32))

    def x3_copy(i, src, slot, to):
        return remote(x3s.at[i, src], x3r.at[i, slot], sent.at[X3 + i], x3_rs.at[i], x_dev(to))

    def x3_wait(i):
        arrived(x3r.at[i, pl.ds(0, 3)], x3_rs.at[i])

    for k in (2, 1, 3):
        x3_copy(0, 0, x, lax.rem(x + k, NX)).start()
    x3r[0, x] = x3s[0, 0]

    gx_forward(1)
    gx_own(2)
    for k in (1, 3, 2):
        for j in (1, 3, 2):
            slot = lax.rem(tp + NT - 2 * j, NT)
            xy_copy(j, 3 - k, slot, slot).wait_recv()
            xc_copy(3 - k, slot).start()
    arrived(xg.at[pl.ds(0, 4)], xc_rs.at[0])

    def columns(t):
        return pl.ds(pl.multiple_of(t * T, T), T)

    xb_v[:, :, columns(x)] = xt_v[x]
    for k in range(1, NX):
        xb_v[:, :, columns(lax.rem(x + k, NX))] = xg[:, k - 1].astype(BF16)

    def rz_copy(h, src, slot, to):
        return remote(dwp.at[h, src], rzr.at[h, slot], sent.at[RZ + h], rz_rs.at[h], z_dev(to))

    def entering(h, t):
        return dot_nt(gx[t, 4:6].reshape(T, DK).astype(BF16), as_v[t, h * DK : (h + 1) * DK].astype(BF16))

    def product(h, t, late):
        vg = (gx[t, 2 * h : 2 * h + 2].reshape(T, DK) + late).astype(BF16)
        return dot(xb_v[:, :, columns(t)].reshape(NZ * ROWS, T), vg)

    def half_product(h):
        mine, late_far = entering(h, x), entering(h, far)
        late_left, late_right = entering(h, left), entering(h, right)
        gx_wait(gx_rest, h + 1)
        near = product(h, x, mine) + product(h, left, late_left) + product(h, right, late_right)
        gx_wait(gx_far, h + 1)
        dwp[h] = (near + product(h, far, late_far)).reshape(NZ, ROWS, DK)
        for k in (4, 3, 5, 2, 6, 1, 7):
            t = lax.rem(z + k, NZ)
            rz_copy(h, t, z, t).start()

    gx_wait(gx_rest, 0)
    gx_wait(gx_far, 0)
    x3_wait(0)
    acc = x3r[0].reshape(DV, DK)
    for t in (3, 2, 1, 0):
        as_v[t] = acc
        if t:
            acc = slab_decay(0, t) * acc
    half_product(0)
    gx_forward(2)
    half_product(1)
    adj_in = adj_row + as_v[x]
    adj_in16 = adj_in.astype(BF16)

    state = jnp.zeros((DV, DK), F32)
    for b in range(NB):
        sl = slice(b * BLK, (b + 1) * BLK)
        locs_v[b] = state.astype(BF16)
        if b < NB - 1:
            state = jnp.exp(ends[b]) * state + dot_tn(v[sl], tail_k[sl])
    out_dots = jnp.where(lower, dot_nt(do, v), 0.0).astype(BF16)
    out_dots_t = jnp.where(upper, dot_nt(v, do), 0.0).astype(BF16)
    local_qg = dot(out_dots, shrunk_k) + jnp.concatenate(
        [dot(do[b * BLK : (b + 1) * BLK], locs_v[b]) for b in range(NB)], axis=0
    )
    local_kg = exp_nc * dot(out_dots_t, grown_q) + exp_tail * jnp.concatenate(
        [dot(v[b * BLK : (b + 1) * BLK], adjs_v[b]) for b in range(NB)], axis=0
    )
    kg = local_kg + to_end * dot(v, adj_in16)
    dk_v[...] = kg.astype(BF16)

    def state_step(t, acc):
        z_copy(1, t, t).wait_recv()
        return z2r[1, t, :SLAB, :] + z2r[1, t, SLAB : SLAB + 1, :] * acc

    acc = lax.fori_loop(0, z, state_step, jnp.zeros((SLAB, DK), F32))
    for t in range(NX):
        x3s[1, t] = acc
        if t < NX - 1:
            acc = slab(1, t) + slab_decay(0, t) * acc
    for k in (2, 1, 3):
        t = lax.rem(x + k, NX)
        x3_copy(1, t, x, t).start()
    x3r[1, x] = x3s[1, x]
    x3_wait(1)
    state_in = x3r[1].reshape(DV, DK)
    qg = exp_c * local_qg + from_start * dot(do, state_in.astype(BF16))
    dq_v[...] = (qg * (DK**-0.5)).astype(BF16)
    carry = jnp.sum(adj_in * (span_state + span_decay * state_in), axis=0, keepdims=True)
    dg_v[...] = exact_sum((col >= row).astype(BF16), qs * qg - kf * kg) + carry
    stores = [
        pltpu.make_async_copy(src, dst, out_sem.at[i])
        for i, (src, dst) in enumerate(((dq_v, dq_o), (dk_v, dk_o), (dg_v, dg_o), (dwo_v, dwo_o), (rn_v, rn_o)))
    ]
    for store in stores[:3]:
        store.start()

    left_here(x1s.at[0, pl.ds(0, 3)], sent.at[X1])
    left_here(x1s.at[1, pl.ds(0, 3), pl.ds(0, SLAB)], sent.at[X1 + 1])
    left_here(z2r.at[0, pl.ds(0, 7)], sent.at[Z2])
    left_here(xis.at[pl.ds(0, 3)], sent.at[XI])
    left_here(x3r.at[0, pl.ds(0, 3)], sent.at[X3])
    left_here(x3r.at[1, pl.ds(0, 3)], sent.at[X3 + 1])
    left_here(gx.at[pl.ds(0, 3)], sent.at[GX])
    left_here(xg, sent.at[XX])
    for store in stores[:3]:
        store.wait()

    squares = jnp.zeros((ROWS, DK), F32)
    for h in range(2):
        part = dwp[h, z]
        arrived(rzr.at[h, pl.ds(0, 7)], rz_rs.at[h])
        for k in range(1, NZ):
            part = part + rzr[h, lax.rem(z + k, NZ)]
        dwo_v[:, h * DK : (h + 1) * DK] = part
        squares = squares + part * part
    stores[3].start()

    norms = jnp.sum(squares.T, axis=0, keepdims=True)
    tps[...] = jnp.broadcast_to(jnp.concatenate([norms, jnp.zeros((1, 64), F32)], axis=1), (8, 128))

    def tp_copy(slot, to):
        return remote(tps, tpr.at[slot], sent.at[TP], tp_rs.at[0], tp_dev(to))

    for k in (4, 5, 3, 2, 6, 7, 1):
        tp_copy(tp, lax.rem(tp + k, NT)).start()
    left_here(dwp.at[0, pl.ds(0, 7)], sent.at[RZ])
    left_here(dwp.at[1, pl.ds(0, 7)], sent.at[RZ + 1])
    stores[3].wait()
    left_here(tpr.at[pl.ds(0, 7)], sent.at[TP])
    arrived(tpr.at[pl.ds(0, 7)], tp_rs.at[0])
    acc = tps[0:1, :]
    for k in range(1, NT):
        t = lax.rem(tp + NT - k, NT)
        acc = acc + tpr[t, 0:1, :]
    rn_v[...] = acc[:, :ROWS]
    stores[4].start()
    stores[4].wait()


def finish(*refs):
    ins, outs, sem = refs[:5], refs[5:10], refs[10]
    copies = [pltpu.make_async_copy(src, dst, sem.at[i]) for i, (src, dst) in enumerate(zip(ins, outs))]
    for cp in copies:
        cp.start()
    for cp in copies:
        cp.wait()


def on_device(block_input, queries, keys, w_value, log_decay, d_out):
    dma, vmem = pltpu.SemaphoreType.DMA, pltpu.VMEM
    hbm_spec = pl.BlockSpec(memory_space=pltpu.HBM)
    shapes = (((T, DK), BF16), ((T, DK), BF16), ((T, DK), F32), ((ROWS, DV), F32), ((1, ROWS), F32))
    args = [
        pltpu.with_memory_space_constraint(a, pltpu.HBM)
        for a in (block_input, queries, keys, w_value, log_decay, d_out)
    ]
    outs = pl.pallas_call(
        kernel,
        out_shape=tuple(vmem(*s) for s in shapes),
        in_specs=[hbm_spec] * 6,
        out_specs=(pl.BlockSpec(memory_space=pl.ANY),) * 5,
        scratch_shapes=[
            vmem((T, 2048), BF16), vmem((T, DK), BF16), vmem((T, DK), BF16),
            vmem((2048, DV), BF16), vmem((T, DK), F32), vmem((T, DV), BF16),
            vmem((T, DK), BF16), vmem((T, DK), BF16), vmem((T, DK), F32),
            vmem((ROWS, DV), F32), vmem((1, ROWS), F32),
            vmem((NX, NZ, ROWS, T), BF16), vmem((T, DV), BF16),
            vmem((NB, DV, DK), BF16), vmem((NB, DV, DK), BF16),
            vmem((NX, DV, DK), F32), vmem((NZ, ROWS, NX * T), BF16),
            vmem((2, NX, SLAB + 8, DK), F32), vmem((2, NX, SLAB + 8, DK), F32),
            vmem((2, SLAB + 8, DK), F32), vmem((2, NZ, SLAB + 8, DK), F32),
            vmem((NX, SLAB, DK), F32), vmem((NX, SLAB, DK), F32),
            vmem((2, NX, SLAB, DK), F32), vmem((2, NX, SLAB, DK), F32),
            vmem((NX, 6, T // 2, DK), F32), vmem((NX, ROWS, T), F32), vmem((NT, NX - 1, ROWS, T), F32),
            vmem((2, NZ, ROWS, DK), F32), vmem((2, NZ, ROWS, DK), F32),
            vmem((8, 128), F32), vmem((NT, 8, 128), F32),
            dma((6,)), dma((5,)), dma((11,)), dma((2,)), dma((NZ,)), dma((1,)), dma((2,)), dma((2, 4)), dma((3,)),
            dma((3,)), dma((3,)), dma((3, 3)), dma((1,)), dma((2,)), dma((1,)),
        ],
        compiler_params=pltpu.CompilerParams(collective_id=0, has_side_effects=True, vmem_limit_bytes=40 << 20),
        name="gla_backward",
    )(*args)
    outs = pl.pallas_call(
        finish,
        out_shape=tuple(jax.ShapeDtypeStruct(*s) for s in shapes),
        in_specs=[pl.BlockSpec(memory_space=pl.ANY)] * 5,
        out_specs=(hbm_spec,) * 5,
        scratch_shapes=[dma((5,))],
        compiler_params=pltpu.CompilerParams(vmem_limit_bytes=1 << 20),
        name="finish",
    )(*outs)
    return (*outs[:4], outs[4].reshape(ROWS))


def solution(mesh):
    in_specs = (P("sp", None), P("sp", "tp"), P("sp", "tp"), P(None, "tp"), P("sp", "tp"), P("sp", "tp"))
    out_specs = (P("sp", "tp"), P("sp", "tp"), P("sp", "tp"), P("sp", "tp"), P("sp"))
    return jax.shard_map(on_device, mesh=mesh, in_specs=in_specs, out_specs=out_specs, check_vma=False)
```
